256 devices in a mesh: sp: 16 (over y, x), tp: 16 (over z, core).
Axes of the slice: x: 4, y: 4, z: 8, core: 2. Of those that a mesh axis runs over, the one named last changes fastest.
Arguments:
- latent: bfloat16 [16384, 2048], P(('sp', 'tp')), may hold values from -1.5 to 1.5
- context: bfloat16 [512, 2048], P('sp'), may hold values from -6 to 6
- cond: bfloat16 [2048], replicated, may hold values from -6 to 6
- cond_context: bfloat16 [2048], replicated, may hold values from -6 to 6
- mod_weight: bfloat16 [3, 2048, 2048], P(None, 'sp', 'tp'), may hold values from -0.125 to 0.125
- norm_gain: bfloat16 [2048], replicated, may hold values from 0.099609375 to 1.8984375
- down_q: bfloat16 [2048, 768], P('tp'), may hold values from -0.125 to 0.125
- down_kv: bfloat16 [2048, 512], P('tp'), may hold values from -0.125 to 0.125
- rope_weight: bfloat16 [2048, 32], replicated, may hold values from -0.125 to 0.125
- qlat_gain: bfloat16 [768], replicated, may hold values from 0.099609375 to 1.8984375
- kvlat_gain: bfloat16 [512], replicated, may hold values from 0.099609375 to 1.8984375
- up_query: bfloat16 [768, 1536], P(None, 'tp'), may hold values from -0.21875 to 0.21875
- up_key: bfloat16 [512, 1024], P(None, 'tp'), may hold values from -0.25 to 0.25
- up_value: bfloat16 [512, 1024], P(None, 'tp'), may hold values from -0.25 to 0.25
- query_gain: float32 [96], replicated, may hold values from 0.5 to 8
- key_gain: float32 [96], replicated, may hold values from 0.5 to 8
- context_bias: float32 [16], P('tp'), may hold values from -2.2 to -0.7
- out_weight: bfloat16 [1024, 2048], P('tp'), may hold values from -48 to 48
Outputs:
- mixed: bfloat16 [16384, 2048], P(('sp', 'tp'))
The draws below stay inside these ranges and needn't reach their ends.
All inputs are finite; a program needn't handle non-finite values.
Results may differ from the reference program's by a relative error of at most 0.028.
The reference program's roundings to bfloat16 on the way count: a program that leaves them out, or rounds other values in their place, can miss the bound.
Values may be sent and summed in bfloat16 or wider, within the bound.
A program may use at most 64 MiB of HBM per device.

```python
import math
import jax
import jax.numpy as jnp
from jax import lax

D = 2048
HEADS = 16
NOPE = 64
ROPE = 32
VDIM = 64
QRANK = 768
KVRANK = 512
GRID_W = 64
TOK_DEV = 1024
CTX_DEV = 32
TOKENS = 16384
CONTEXT = 512


def draw_gain_vector(key):
    return jax.random.uniform(key, (NOPE + ROPE,), jnp.float32, 1.1, 1.9)


def draw_query_gain(key, part):
    return draw_gain_vector(jax.random.fold_in(key, 11))


def draw_key_gain(key, part):
    return draw_gain_vector(jax.random.fold_in(key, 23))


def level_of(own_key, shape, cuts, smallest, largest):
    level = 1.0
    for position, blocks in cuts:
        heights = jax.random.uniform(jax.random.fold_in(jax.random.fold_in(own_key, 6), position), (blocks,), jnp.float32, smallest / len(cuts), largest / len(cuts))
        level = level * jnp.repeat(jnp.exp(heights), shape[position] // blocks).reshape((-1,) + (1,) * (len(shape) - 1 - position))
    return level


def bell_draw(own_key, shape, deviation, bound, cuts=(), held_as=jnp.bfloat16):
    level = level_of(own_key, shape, cuts, -0.22, 0.18) if cuts else 1.0
    result = jax.random.normal(own_key, shape, jnp.float32) * deviation * level
    return jnp.minimum(jnp.maximum(result, -bound), bound).astype(held_as)


def setup_inputs(seed: int = 0) -> dict:
    streams_of = jax.random.split(jax.random.key(seed), 19)
    latent = bell_draw(streams_of[0], (TOKENS, D), 0.25, 1.5, ((0, 256),))
    context = bell_draw(streams_of[1], (CONTEXT, D), 1.0, 6.0, ((0, 16),))
    cond = bell_draw(streams_of[2], (D,), 1.0, 6.0)
    cond_context = bell_draw(streams_of[3], (D,), 1.0, 6.0)
    mod_weight = bell_draw(streams_of[4], (3, D, D), D ** -0.5, 0.125, ((1, 16), (2, 16)))
    norm_gain = jnp.clip(1.0 + 0.18 * jax.random.normal(streams_of[5], (D,), jnp.float32), 0.099609375, 1.8984375).astype(jnp.bfloat16)
    down_q = bell_draw(streams_of[6], (D, QRANK), D ** -0.5, 0.125, ((0, 16),))
    down_kv = bell_draw(streams_of[7], (D, KVRANK), D ** -0.5, 0.125, ((0, 16),))
    rope_weight = bell_draw(streams_of[8], (D, ROPE), D ** -0.5, 0.125)
    qlat_gain = jnp.clip(1.0 + 0.18 * jax.random.normal(streams_of[9], (QRANK,), jnp.float32), 0.099609375, 1.8984375).astype(jnp.bfloat16)
    kvlat_gain = jnp.clip(1.0 + 0.18 * jax.random.normal(streams_of[10], (KVRANK,), jnp.float32), 0.099609375, 1.8984375).astype(jnp.bfloat16)
    up_query = bell_draw(streams_of[11], (QRANK, HEADS * (NOPE + ROPE)), QRANK ** -0.5, 0.21875, ((1, 16),))
    up_key = bell_draw(streams_of[12], (KVRANK, HEADS * NOPE), KVRANK ** -0.5, 0.25, ((1, 16),))
    up_value = bell_draw(streams_of[13], (KVRANK, HEADS * VDIM), KVRANK ** -0.5, 0.25, ((1, 16),))
    query_gain = draw_query_gain(jax.random.fold_in(streams_of[18], 71), 0)
    key_gain = draw_key_gain(jax.random.fold_in(streams_of[18], 71), 0)
    context_bias = jnp.clip(-2.2 + 1.5 * jax.random.uniform(streams_of[16], (HEADS,), jnp.float32) ** level_of(streams_of[16], (HEADS,), ((0, 16),), -0.2, 0.2), -2.2, -0.7)
    out_weight = bell_draw(streams_of[17], (HEADS * VDIM, D), (2.0 * (TOKENS + CONTEXT) ** 0.5 * (HEADS * VDIM) ** -0.5), 48.0, ((0, 16),))
    return dict(latent=latent, context=context, cond=cond, cond_context=cond_context, mod_weight=mod_weight, norm_gain=norm_gain, down_q=down_q, down_kv=down_kv, rope_weight=rope_weight, qlat_gain=qlat_gain, kvlat_gain=kvlat_gain, up_query=up_query, up_key=up_key, up_value=up_value, query_gain=query_gain, key_gain=key_gain, context_bias=context_bias, out_weight=out_weight)


epsilon = 1e-06
theta = 10000.0

def rounded(tensor):
    return lax.optimization_barrier(tensor.astype(jnp.bfloat16))

def rms_scale(tensor, gain):
    return tensor * lax.rsqrt(lax.optimization_barrier(jnp.mean(tensor * tensor, axis=-1, keepdims=True)) + epsilon) * gain.astype(jnp.float32)

def axial_tables(positions):
    pair_count = ROPE // 4
    frequency = jnp.power(theta, -jnp.arange(pair_count, dtype=jnp.float32) / pair_count)
    row_angle = (positions // GRID_W).astype(jnp.float32)[:, None] * frequency
    col_angle = (positions % GRID_W).astype(jnp.float32)[:, None] * frequency
    return (jnp.cos(row_angle), jnp.sin(row_angle), jnp.cos(col_angle), jnp.sin(col_angle))

def rotate_half(tensor, cosine, sine_table):
    first, second = jnp.split(tensor, 2, axis=-1)
    cosine = cosine[:, None, :]
    sine_table = sine_table[:, None, :]
    return jnp.concatenate([first * cosine - second * sine_table, second * cosine + first * sine_table], axis=-1)

def axial_rotate(tensor, tables):
    half_width = tensor.shape[-1] // 2
    return jnp.concatenate([rotate_half(tensor[..., :half_width], tables[0], tables[1]), rotate_half(tensor[..., half_width:], tables[2], tables[3])], axis=-1)

def modulate(row_block, gain, shifts, scales):
    normal = rms_scale(row_block.astype(jnp.float32), gain)
    return rounded(normal * (1.0 + scales) + shifts)

def make_queries(query_latent, up_query, query_gain, tables):
    amount = query_latent.shape[0]
    projected = jnp.dot(query_latent, up_query, preferred_element_type=jnp.float32).reshape(amount, -1, NOPE + ROPE)
    normal = rms_scale(projected, query_gain)
    return rounded(jnp.concatenate([normal[..., :NOPE], axial_rotate(normal[..., NOPE:], tables)], axis=-1))

def make_keys(kv_latent, rope_rows, up_key, up_value, key_gain, tables):
    amount = kv_latent.shape[0]
    unrotated = jnp.dot(kv_latent, up_key, preferred_element_type=jnp.float32).reshape(amount, -1, NOPE)
    head_count = unrotated.shape[1]
    shared = jnp.broadcast_to(rope_rows.astype(jnp.float32)[:, None, :], (amount, head_count, ROPE))
    normal = rms_scale(jnp.concatenate([unrotated, shared], axis=-1), key_gain)
    if tables is not None:
        normal = jnp.concatenate([normal[..., :NOPE], axial_rotate(normal[..., NOPE:], tables)], axis=-1)
    values = jnp.dot(kv_latent, up_value, preferred_element_type=jnp.float32).reshape(amount, head_count, VDIM)
    return (rounded(normal), rounded(values))

def attend(query_block, keys, values, context_keys, context_values, context_shift):
    scaling = (NOPE + ROPE) ** (-0.5)
    query_wide = query_block.astype(jnp.float32)
    latent_scores = jnp.einsum('qhd,khd->qhk', query_wide, keys.astype(jnp.float32)) * scaling
    context_scores = jnp.einsum('qhd,khd->qhk', query_wide, context_keys.astype(jnp.float32)) * scaling
    context_scores = context_scores + context_shift[None, :, None]
    row_max = jnp.maximum(lax.optimization_barrier(jnp.max(latent_scores, axis=-1)), lax.optimization_barrier(jnp.max(context_scores, axis=-1)))[..., None]
    latent_weights = jnp.exp(latent_scores - row_max)
    context_weights = jnp.exp(context_scores - row_max)
    totals = lax.optimization_barrier(jnp.sum(latent_weights, axis=-1)) + lax.optimization_barrier(jnp.sum(context_weights, axis=-1))
    summed = jnp.einsum('qhk,khd->qhd', rounded(latent_weights).astype(jnp.float32), values.astype(jnp.float32))
    summed = summed + jnp.einsum('qhk,khd->qhd', rounded(context_weights).astype(jnp.float32), context_values.astype(jnp.float32))
    return rounded(summed / totals[..., None])

def reference(latent, context, cond, cond_context, mod_weight, norm_gain, down_q, down_kv, rope_weight, qlat_gain, kvlat_gain, up_query, up_key, up_value, query_gain, key_gain, context_bias, out_weight):
    activated = rounded(jax.nn.silu(jnp.stack([cond, cond_context]).astype(jnp.float32)))
    shifts, scales, gates = (jnp.dot(activated[0], mod_weight[member], preferred_element_type=jnp.float32) for member in range(3))
    context_shift, context_scale = (jnp.dot(activated[1], mod_weight[member], preferred_element_type=jnp.float32) for member in range(2))
    normed = modulate(latent, norm_gain, shifts, scales)
    context_normed = modulate(context, norm_gain, context_shift, context_scale)
    query_latent = rounded(rms_scale(jnp.dot(normed, down_q, preferred_element_type=jnp.float32), qlat_gain))
    kv_latent = rounded(rms_scale(jnp.dot(normed, down_kv, preferred_element_type=jnp.float32), kvlat_gain))
    context_kv = rounded(rms_scale(jnp.dot(context_normed, down_kv, preferred_element_type=jnp.float32), kvlat_gain))
    rope_rows = rounded(jnp.dot(normed, rope_weight, preferred_element_type=jnp.float32))
    context_rope = rounded(jnp.dot(context_normed, rope_weight, preferred_element_type=jnp.float32))
    tables = axial_tables(jnp.arange(TOKENS, dtype=jnp.int32))
    queries = make_queries(query_latent, up_query, query_gain, tables)
    keys, values = make_keys(kv_latent, rope_rows, up_key, up_value, key_gain, tables)
    context_keys, context_values = make_keys(context_kv, context_rope, up_key, up_value, key_gain, None)
    context_shift_heads = context_bias.astype(jnp.float32) + math.log(TOK_DEV / CTX_DEV)
    block_rows = math.gcd(TOKENS, 256)
    query_blocks = queries.reshape(TOKENS // block_rows, block_rows, HEADS, NOPE + ROPE)
    attended = lax.map(lambda blocks: attend(blocks, keys, values, context_keys, context_values, context_shift_heads), query_blocks)
    attended = attended.reshape(TOKENS, HEADS * VDIM)
    projected = jnp.dot(attended, out_weight, preferred_element_type=jnp.float32)
    return (latent.astype(jnp.float32) + gates * projected).astype(jnp.bfloat16)
```

```python
import functools
import math

import jax
import jax.numpy as jnp
from jax import lax
from jax.experimental import pallas as pl
from jax.experimental.pallas import tpu as pltpu
from jax.sharding import PartitionSpec as P

NOPE = 64
ROPE = 32
HEAD = NOPE + ROPE
VDIM = 64
GRID_W = 64
TOK_DEV = 1024
CTX_DEV = 32
D = 2048
SP_TP = ("sp", "tp")
BF = jnp.bfloat16
F32 = jnp.float32

epsilon = 1e-06
theta = 10000.0
SCALE2 = math.log2(math.e) * HEAD ** (-0.5)
LOG2E = math.log2(math.e)


def exchange_items():
    items = {}
    for h in (0, 1):
        def add(da, db, part, axis, step, trigger):
            names = ("x", "y") if h == 0 else ("y", "x")
            items[(h, da, db, part)] = (names[axis], step, trigger)
        add(-1, 0, "U", 0, 1, None)
        add(1, 0, "U", 0, -1, None)
        add(2, 0, 0, 0, 1, (h, -1, 0, "U"))
        add(2, 0, 1, 0, -1, (h, 1, 0, "U"))
        for da in (0, -1, 1):
            trigger = None if da == 0 else (h, da, 0, "U")
            add(da, -1, "U", 1, 1, trigger)
            add(da, 1, "U", 1, -1, trigger)
            add(da, 2, 0, 1, 1, (h, da, -1, "U"))
            add(da, 2, 1, 1, -1, (h, da, 1, "U"))
        for q in (0, 1):
            add(2, -1, q, 1, 1, (h, 2, 0, q))
            add(2, 1, q, 1, -1, (h, 2, 0, q))
        add(2, 2, 0, 1, 1, (h, 2, -1, 0))
        add(2, 2, 1, 1, -1, (h, 2, 1, 1))
    return items


def arrival_times(items, unit=3.53, latency=1.8):
    free, arrive = {}, {}
    waiting = []
    for n, (key, (axis, step, trigger)) in enumerate(items.items()):
        if trigger is None:
            first = axis == ("x" if key[0] == 0 else "y")
            waiting.append((0.0, 0 if first else 1, n, key))
    count = len(items)
    while waiting:
        waiting.sort()
        at, _, _, key = waiting.pop(0)
        axis, step, _ = items[key]
        span = unit if key[3] == "U" else unit / 2
        begin = max(at, free.get((axis, step), 0.0))
        free[(axis, step)] = begin + span
        arrive[key] = begin + span + latency
        for other, (_, _, trigger) in items.items():
            if trigger == key:
                count += 1
                waiting.append((arrive[key], 0, count, other))
    return arrive


ITEMS = exchange_items()
ARRIVE = arrival_times(ITEMS)
ITEM_ORDER = sorted(ITEMS, key=lambda k: (round(ARRIVE[k], 1), str(k)))
ITEM_INDEX = {k: n for n, k in enumerate(ITEM_ORDER)}


def unit_order():
    ready = {}
    for k in ITEM_ORDER:
        ready[k[:3]] = max(ready.get(k[:3], 0.0), ARRIVE[k])
    units = sorted(ready, key=lambda u: (round(ready[u], 1), str(u)))
    return [(0, 0, 0), (1, 0, 0)] + units


UNITS = unit_order()
SLOT = {u: n for n, u in enumerate(UNITS)}
N_UNITS = len(UNITS) + 1
CTX_SLOT = len(UNITS)


def item_steps(per_step=0.62):
    steps = {}
    now = 0.0
    placed = set()
    plan = []
    for n in range(N_UNITS):
        need = []
        if n < len(UNITS):
            need = [k for k in ITEM_ORDER if k[:3] == UNITS[n] and k not in placed]
        for k in need:
            now = max(now, ARRIVE[k])
        early = [k for k in ITEM_ORDER if k not in placed and (k in need or ARRIVE[k] <= now)]
        placed.update(early)
        plan.append(early)
        now += per_step
    return plan


PLAN = item_steps()


class Board:
    def __init__(self, sends, recvs):
        self.sends, self.recvs, self.count, self.started = sends, recvs, 0, []

    def take(self, n=1):
        first = self.count
        self.count += n
        return first

    def send(self, number, src, dst, device):
        copy = pltpu.make_async_remote_copy(
            src_ref=src, dst_ref=dst, send_sem=self.sends.at[number],
            recv_sem=self.recvs.at[number], device_id=device,
            device_id_type=pl.DeviceIdType.MESH)
        copy.start()

    def arrived(self, number, dst, device):
        pltpu.make_async_remote_copy(
            src_ref=dst, dst_ref=dst, send_sem=self.sends.at[number],
            recv_sem=self.recvs.at[number], device_id=device,
            device_id_type=pl.DeviceIdType.MESH).wait_recv()

    def sent(self, number, src, device):
        pltpu.make_async_remote_copy(
            src_ref=src, dst_ref=src, send_sem=self.sends.at[number],
            recv_sem=self.recvs.at[number], device_id=device,
            device_id_type=pl.DeviceIdType.MESH).wait_send()


class Place:
    def __init__(self):
        self.s = lax.axis_index("sp")
        self.t = lax.axis_index("tp")
        self.y, self.x = self.s // 4, self.s % 4
        self.z, self.c = self.t // 2, self.t % 2

    def plane(self, axis, step):
        y, x = self.y, self.x
        if axis == "x":
            x = (x + step + 4) % 4
        else:
            y = (y + step + 4) % 4
        return {"sp": y * 4 + x, "tp": self.t}

    def sp_peer(self, k):
        return {"sp": (self.s + k) % 16, "tp": self.t}

    def tp_peer(self, k):
        return {"sp": self.s, "tp": (self.t + k) % 16}

    def ring(self, step):
        return {"sp": self.s, "tp": ((self.z + step + 8) % 8) * 2 + self.c}

    def sibling(self):
        return {"sp": self.s, "tp": self.z * 2 + 1 - self.c}


def greet(devices):
    barrier = pltpu.get_barrier_semaphore()
    for device in devices:
        pl.semaphore_signal(barrier, inc=1, device_id=device,
                            device_id_type=pl.DeviceIdType.MESH)
    pl.semaphore_wait(barrier, len(devices))


class ZRing:
    def __init__(self, board, place, own, bufs):
        self.board, self.place, self.own, self.bufs = board, place, own, bufs
        self.base = board.take(16)

    def number(self, way, dist, part):
        return self.base + (0 if way == 1 else 8) + (dist - 1) * 2 + part

    def slot(self, way, dist, part):
        return self.bufs[part].at[(self.place.z - way * dist + 16) % 8]

    def begin(self):
        for part in (0, 1):
            for way in (1, -1):
                self.board.send(self.number(way, 1, part), self.own[part],
                                self.bufs[part].at[self.place.z], self.place.ring(way))

    def take(self, way, dist, part):
        here = self.slot(way, dist, part)
        self.board.arrived(self.number(way, dist, part), here, self.place.ring(-way))
        if dist < 3 or (dist == 3 and part == (0 if way == 1 else 1)):
            self.board.send(self.number(way, dist + 1, part), here, here, self.place.ring(way))

    def items(self):
        out = []
        for dist in (1, 2, 3):
            for part in (0, 1):
                for way in (1, -1):
                    out.append((way, dist, part))
        out.append((1, 4, 0))
        out.append((-1, 4, 1))
        return out

    def drain(self):
        for part in (0, 1):
            for way in (1, -1):
                self.board.sent(self.number(way, 1, part), self.own[part], self.place.ring(way))
        for way, dist, part in self.items():
            if dist > 1:
                here = self.slot(way, dist - 1, part)
                self.board.sent(self.number(way, dist, part), here, self.place.ring(way))


def quarter_ref(buf, slot, part):
    if part == "U":
        return buf.at[slot]
    return buf.at[slot, part]


def attention_kernel(qt_ref, kvt_ref, ctx_ref, bias_ref, ow_ref, lat_ref, gate_ref, out_ref,
                     kvb, cbuf, owa, owb, s_a, s_b, mb_a, mb_b, m_ref, l_ref, acc, att, attb,
                     part_ref, sib_ref, sends, recvs):
    place = Place()
    board = Board(sends, recvs)
    kv_base = board.take(len(ITEM_ORDER))
    ctx_base = board.take(16)
    a2a_base = board.take(8)
    d2d = board.take(1)
    half_cols = D // 2
    ring = ZRing(board, place, (ow_ref.at[:, :half_cols], ow_ref.at[:, half_cols:]), (owa, owb))

    greet([place.sp_peer(k) for k in range(1, 16)] + [place.ring(k) for k in range(1, 8)]
          + [place.sibling()])

    def kv_send(key, src):
        axis, step, _ = ITEMS[key]
        h, da, db, part = key
        board.send(kv_base + ITEM_INDEX[key], src, quarter_ref(kvb, SLOT[key[:3]], part),
                   place.plane(axis, step))

    def own_part(h):
        return kvt_ref.at[h]

    for key in sorted((k for k in ITEMS if ITEMS[k][2] is None),
                      key=lambda k: 0 if ITEMS[k][0] == ("x" if k[0] == 0 else "y") else 1):
        kv_send(key, own_part(key[0]))
    ring.begin()
    for k in range(1, 16):
        board.send(ctx_base + k, ctx_ref, cbuf.at[place.s], place.sp_peer(k))
    cbuf[place.s] = ctx_ref[...]
    owa[place.z] = ow_ref[:, :half_cols]
    owb[place.z] = ow_ref[:, half_cols:]
    kvb[0] = kvt_ref[0]
    kvb[1] = kvt_ref[1]

    def kv_take(key):
        axis, step, _ = ITEMS[key]
        here = quarter_ref(kvb, SLOT[key[:3]], key[3])
        board.arrived(kv_base + ITEM_INDEX[key], here, place.plane(axis, -step))
        for other in ITEM_ORDER:
            if ITEMS[other][2] == key:
                src = here
                if key[3] == "U" and other[3] != "U":
                    src = kvb.at[SLOT[key[:3]], other[3]]
                kv_send(other, src)

    def ctx_unit():
        for k in range(1, 16):
            board.arrived(ctx_base + k, cbuf.at[(place.s - k + 16) % 16], place.sp_peer(16 - k))
        turned = cbuf[...].reshape(512, 256).astype(F32).T.astype(BF)
        for q in (0, 1):
            kvb[CTX_SLOT, q, 0:HEAD, :] = turned[0:HEAD, q * 256:(q + 1) * 256]
            kvb[CTX_SLOT, q, HEAD:HEAD + VDIM, :] = turned[128:128 + VDIM, q * 256:(q + 1) * 256]

    m_ref[...] = jnp.full(m_ref.shape, -jnp.inf, F32)
    l_ref[...] = jnp.zeros(l_ref.shape, F32)
    acc[...] = jnp.zeros(acc.shape, F32)

    def products(slot, s_ref, mb_ref):
        for q in (0, 1):
            keys = kvb[slot, q, 0:128, :].T
            for n in range(4):
                cols = slice(n * 256, (n + 1) * 256)
                scores = jnp.dot(keys, qt_ref[:, cols], preferred_element_type=F32)
                s_ref[q * 256:(q + 1) * 256, cols] = scores
                top = jnp.max(scores, axis=0, keepdims=True)
                mb_ref[:, cols] = top if q == 0 else jnp.maximum(mb_ref[:, cols], top)

    def absorb(slot, s_ref, mb_ref, bias):
        for n in range(4):
            cols = slice(n * 256, (n + 1) * 256)
            old = m_ref[:, cols]
            top = mb_ref[:, cols] * SCALE2
            if bias is not None:
                top = top + bias
            new = jnp.maximum(old, top)
            m_ref[:, cols] = new
            factor = jnp.exp2(old - new)
            less = new if bias is None else new - bias
            weights = jnp.exp2(s_ref[:, cols] * SCALE2 - less)
            l_ref[:, cols] = l_ref[:, cols] * factor + jnp.sum(weights, axis=0, keepdims=True)
            rounded = weights.astype(BF)
            summed = jnp.dot(kvb[slot, 0, HEAD:HEAD + VDIM, :], rounded[:256],
                             preferred_element_type=F32)
            summed = summed + jnp.dot(kvb[slot, 1, HEAD:HEAD + VDIM, :], rounded[256:],
                                      preferred_element_type=F32)
            acc[:, cols] = acc[:, cols] * factor + summed

    ring_items = ring.items()
    ring_plan = [[] for _ in range(N_UNITS)]
    for n, item in enumerate(ring_items):
        ring_plan[min(4 + (n * 26) // len(ring_items), N_UNITS - 1)].append(item)

    def actions(n):
        for key in PLAN[n]:
            kv_take(key)
        for item in ring_plan[n]:
            ring.take(*item)
        if n == CTX_SLOT:
            ctx_unit()

    def act_in_loop(i, offset):
        for trip in range(16):
            n = 2 * trip + offset
            if PLAN[n] or ring_plan[n] or n == CTX_SLOT:
                @pl.when(i == trip)
                def _():
                    actions(n)

    actions(0)
    products(0, s_a, mb_a)

    def body(i, carry):
        act_in_loop(i, 1)
        products(2 * i + 1, s_b, mb_b)
        absorb(2 * i, s_a, mb_a, None)
        act_in_loop(i, 2)
        products(2 * i + 2, s_a, mb_a)
        absorb(2 * i + 1, s_b, mb_b, None)
        return carry

    lax.fori_loop(0, 16, body, 0)
    bias = (bias_ref[0, 0] + math.log(TOK_DEV / CTX_DEV)) * LOG2E
    absorb(CTX_SLOT, s_a, mb_a, bias)

    for k in range(8):
        cols = slice(k * 128, (k + 1) * 128)
        att[k] = (acc[:, cols] / l_ref[:, cols]).astype(BF)
    for k in range(1, 8):
        board.send(a2a_base + k, att.at[(place.z + k) % 8], attb.at[place.z], place.ring(k))
    attb[place.z] = att[place.z]
    for k in range(1, 8):
        board.arrived(a2a_base + k, attb.at[(place.z - k + 8) % 8], place.ring(-k))
    rows = attb[...].reshape(8 * VDIM, 128).astype(F32).T.astype(BF)
    for n, weight in enumerate((owa, owb)):
        part_ref[:, n * half_cols:(n + 1) * half_cols] = jnp.dot(
            rows, weight[...].reshape(8 * VDIM, half_cols), preferred_element_type=F32)
    away = part_ref.at[pl.ds(pl.multiple_of(64 * (1 - place.c), 64), 64)]
    board.send(d2d, away, sib_ref, place.sibling())
    board.arrived(d2d, sib_ref, place.sibling())
    mine = part_ref[pl.ds(pl.multiple_of(64 * place.c, 64), 64)]
    projected = mine + sib_ref[...]
    out_ref[...] = (lat_ref[...].astype(F32) + gate_ref[...] * projected).astype(BF)

    board.sent(d2d, away, place.sibling())
    for k in range(1, 8):
        board.sent(a2a_base + k, att.at[(place.z + k) % 8], place.ring(k))
    for k in range(1, 16):
        board.sent(ctx_base + k, ctx_ref, place.sp_peer(k))
    ring.drain()
    for key in ITEM_ORDER:
        axis, step, _ = ITEMS[key]
        src = quarter_ref(kvb, 0, key[3])
        board.sent(kv_base + ITEM_INDEX[key], src, place.plane(axis, step))


def attention(qt, kvt, ctx, bias, out_weight, latent, gates):
    vmem = pl.BlockSpec(memory_space=pltpu.VMEM)
    copies = len(ITEM_ORDER) + 16 + 8 + 1 + 16
    return pl.pallas_call(
        attention_kernel,
        out_shape=jax.ShapeDtypeStruct((64, D), BF),
        in_specs=[vmem, vmem, vmem, pl.BlockSpec(memory_space=pltpu.SMEM), vmem, vmem, vmem],
        out_specs=vmem,
        scratch_shapes=[
            pltpu.VMEM((N_UNITS, 2, HEAD + VDIM, 256), BF),
            pltpu.VMEM((16, CTX_DEV, 256), BF),
            pltpu.VMEM((8, 64, D // 2), BF),
            pltpu.VMEM((8, 64, D // 2), BF),
            pltpu.VMEM((512, 1024), F32),
            pltpu.VMEM((512, 1024), F32),
            pltpu.VMEM((1, 1024), F32),
            pltpu.VMEM((1, 1024), F32),
            pltpu.VMEM((1, 1024), F32),
            pltpu.VMEM((1, 1024), F32),
            pltpu.VMEM((VDIM, 1024), F32),
            pltpu.VMEM((8, VDIM, 128), BF),
            pltpu.VMEM((8, VDIM, 128), BF),
            pltpu.VMEM((128, D), F32),
            pltpu.VMEM((64, D), F32),
            pltpu.SemaphoreType.DMA((copies,)),
            pltpu.SemaphoreType.DMA((copies,)),
        ],
        compiler_params=pltpu.CompilerParams(collective_id=0, has_side_effects=True,
                                             vmem_limit_bytes=50 * 1024 * 1024),
        cost_estimate=pl.CostEstimate(flops=6 * 10**9, bytes_accessed=10**7,
                                      transcendentals=17 * 10**6),
        name="attention",
    )(qt, kvt, ctx, bias, out_weight, latent, gates)


def sent_together(arrays, axis, dim, along):
    ends, at = ([], 0)
    for a in arrays[:-1]:
        at += a.shape[along]
        ends.append(at)
    both = jnp.concatenate(arrays, axis=along)
    return tuple(jnp.split(lax.all_gather(both, axis, axis=dim, tiled=True), ends, axis=along))


def rms_scale(tensor, gain):
    return (
        tensor
        * lax.rsqrt(jnp.mean(tensor * tensor, axis=-1, keepdims=True) + epsilon)
        * gain.astype(jnp.float32)
    )


def axial_tables(positions):
    pair_count = ROPE // 4
    frequency = jnp.power(theta, -jnp.arange(pair_count, dtype=jnp.float32) / pair_count)
    row_angle = (positions // GRID_W).astype(jnp.float32)[:, None] * frequency
    col_angle = (positions % GRID_W).astype(jnp.float32)[:, None] * frequency
    return (jnp.cos(row_angle), jnp.sin(row_angle), jnp.cos(col_angle), jnp.sin(col_angle))


def rotate_half(tensor, cosine, sine_table):
    first, second = jnp.split(tensor, 2, axis=-1)
    return jnp.concatenate(
        [first * cosine - second * sine_table, second * cosine + first * sine_table], axis=-1
    )


def axial_rotate(tensor, tables):
    half_width = tensor.shape[-1] // 2
    return jnp.concatenate(
        [
            rotate_half(tensor[..., :half_width], tables[0], tables[1]),
            rotate_half(tensor[..., half_width:], tables[2], tables[3]),
        ],
        axis=-1,
    )


def modulate(row_block, gain, shifts, scales):
    normal = rms_scale(row_block.astype(jnp.float32), gain)
    return (normal * (1.0 + scales) + shifts).astype(jnp.bfloat16)


def make_queries(query_latent, up_query, query_gain, tables):
    projected = jnp.dot(query_latent, up_query, preferred_element_type=jnp.float32)
    normal = rms_scale(projected, query_gain)
    return jnp.concatenate(
        [normal[..., :NOPE], axial_rotate(normal[..., NOPE:], tables)], axis=-1
    ).astype(jnp.bfloat16)


def make_keys(kv_latent, rope_rows, up_key, up_value, key_gain, tables):
    unrotated = jnp.dot(kv_latent, up_key, preferred_element_type=jnp.float32)
    normal = rms_scale(jnp.concatenate([unrotated, rope_rows.astype(F32)], axis=-1), key_gain)
    if tables is not None:
        normal = jnp.concatenate(
            [normal[..., :NOPE], axial_rotate(normal[..., NOPE:], tables)], axis=-1
        )
    values = jnp.dot(kv_latent, up_value, preferred_element_type=jnp.float32)
    return (normal.astype(jnp.bfloat16), values.astype(jnp.bfloat16))


def shards(
    latent,
    context,
    cond,
    cond_context,
    mod_weight,
    norm_gain,
    down_q,
    down_kv,
    rope_weight,
    qlat_gain,
    kvlat_gain,
    up_query,
    up_key,
    up_value,
    query_gain,
    key_gain,
    context_bias,
    out_weight,
):
    seq_index = lax.axis_index("sp")
    tp_count = lax.axis_size("tp")
    own_rows = latent.shape[0]
    block_tokens = own_rows * tp_count
    row_span = mod_weight.shape[1]
    activated = jax.nn.silu(jnp.stack([cond, cond_context]).astype(jnp.float32)).astype(
        jnp.bfloat16
    )
    own_part = lax.dynamic_slice_in_dim(activated, seq_index * row_span, row_span, 1)
    partial_value = jnp.concatenate(
        [
            jnp.einsum("d,rde->re", own_part[0], mod_weight, preferred_element_type=jnp.float32),
            jnp.einsum(
                "d,rde->re", own_part[1], mod_weight[:2], preferred_element_type=jnp.float32
            ),
        ],
        axis=0,
    )
    summed = lax.psum(partial_value, "sp")
    modulations = lax.all_gather(summed, "tp", axis=1, tiled=True)
    normed = modulate(latent, norm_gain, modulations[0], modulations[1])
    context_normed = modulate(context, norm_gain, modulations[3], modulations[4])
    stacked = jnp.concatenate([normed, context_normed], axis=0)
    pieces = sent_together((down_q, down_kv), "tp", 0, 1)
    query_down = jnp.dot(stacked[:own_rows], pieces[0], preferred_element_type=jnp.float32)
    kv_down = jnp.dot(stacked, pieces[1], preferred_element_type=jnp.float32)
    query_latent = rms_scale(query_down, qlat_gain).astype(jnp.bfloat16)
    kv_latent = rms_scale(kv_down, kvlat_gain).astype(jnp.bfloat16)
    rope_rows = jnp.dot(stacked, rope_weight, preferred_element_type=jnp.float32).astype(
        jnp.bfloat16
    )
    all_query, all_kv, all_rope = sent_together(
        (query_latent, kv_latent[:own_rows], rope_rows[:own_rows]), "tp", 0, 1
    )
    ck, cv = make_keys(
        kv_latent[own_rows:], rope_rows[own_rows:], up_key, up_value, key_gain, None
    )
    positions = seq_index * block_tokens + jnp.arange(block_tokens, dtype=jnp.int32)
    tables = axial_tables(positions)
    queries = make_queries(all_query, up_query, query_gain, tables)
    keys, values = make_keys(all_kv, all_rope, up_key, up_value, key_gain, tables)
    qt = jnp.pad(queries, ((0, 0), (0, 128 - HEAD))).T
    kvt = jnp.concatenate([keys, values], axis=1).T
    kvt = kvt.reshape(HEAD + VDIM, 2, 2, 256).transpose(1, 2, 0, 3)
    ctx = jnp.concatenate(
        [jnp.pad(ck, ((0, 0), (0, 128 - HEAD))), jnp.pad(cv, ((0, 0), (0, 128 - VDIM)))], axis=1
    )
    gates = modulations[2:3]
    return attention(qt, kvt, ctx, context_bias.reshape(1, 1), out_weight, latent, gates)


def solution(mesh):
    placed = (
        P(SP_TP, None),
        P("sp", None),
        P(),
        P(),
        P(None, "sp", "tp"),
        P(),
        P("tp", None),
        P("tp", None),
        P(),
        P(),
        P(),
        P(None, "tp"),
        P(None, "tp"),
        P(None, "tp"),
        P(),
        P(),
        P("tp"),
        P("tp", None),
    )
    return jax.shard_map(
        shards, mesh=mesh, in_specs=placed, out_specs=P(SP_TP, None), check_vma=False
    )
```

```python
import math

import jax
import jax.numpy as jnp
import numpy as np
from jax import lax
from jax.experimental import pallas as pl
from jax.experimental.pallas import tpu as pltpu
from jax.sharding import PartitionSpec as P

NOPE = 64
ROPE = 32
HEAD = NOPE + ROPE
VDIM = 64
GRID_W = 64
TOK_DEV = 1024
CTX_DEV = 32
D = 2048
SP_TP = ("sp", "tp")
BF = jnp.bfloat16
F32 = jnp.float32

epsilon = 1e-06
theta = 10000.0
SCALE2 = math.log2(math.e) * HEAD ** (-0.5)
LOG2E = math.log2(math.e)


def exchange_items():
    items = {}
    for h in (0, 1):
        def add(da, db, part, axis, step, trigger):
            names = ("x", "y") if h == 0 else ("y", "x")
            items[(h, da, db, part)] = (names[axis], step, trigger)
        add(-1, 0, "U", 0, 1, None)
        add(1, 0, "U", 0, -1, None)
        add(2, 0, 0, 0, 1, (h, -1, 0, "U"))
        add(2, 0, 1, 0, -1, (h, 1, 0, "U"))
        for da in (0, -1, 1):
            trigger = None if da == 0 else (h, da, 0, "U")
            add(da, -1, "U", 1, 1, trigger)
            add(da, 1, "U", 1, -1, trigger)
            add(da, 2, 0, 1, 1, (h, da, -1, "U"))
            add(da, 2, 1, 1, -1, (h, da, 1, "U"))
        for q in (0, 1):
            add(2, -1, q, 1, 1, (h, 2, 0, q))
            add(2, 1, q, 1, -1, (h, 2, 0, q))
        add(2, 2, 0, 1, 1, (h, 2, -1, 0))
        add(2, 2, 1, 1, -1, (h, 2, 1, 1))
    return items


def arrival_times(items, unit=3.53, latency=1.8):
    free, arrive = {}, {}
    waiting = []
    for n, (key, (axis, step, trigger)) in enumerate(items.items()):
        if trigger is None:
            first = axis == ("x" if key[0] == 0 else "y")
            waiting.append((0.0, 0 if first else 1, n, key))
    count = len(items)
    while waiting:
        waiting.sort()
        at, _, _, key = waiting.pop(0)
        axis, step, _ = items[key]
        span = unit if key[3] == "U" else unit / 2
        begin = max(at, free.get((axis, step), 0.0))
        free[(axis, step)] = begin + span
        arrive[key] = begin + span + latency
        for other, (_, _, trigger) in items.items():
            if trigger == key:
                count += 1
                waiting.append((arrive[key], 0, count, other))
    return arrive


ITEMS = exchange_items()
ARRIVE = arrival_times(ITEMS)
ITEM_ORDER = sorted(ITEMS, key=lambda k: (round(ARRIVE[k], 1), str(k)))
ITEM_INDEX = {k: n for n, k in enumerate(ITEM_ORDER)}


def unit_order():
    ready = {}
    for k in ITEM_ORDER:
        ready[k[:3]] = max(ready.get(k[:3], 0.0), ARRIVE[k])
    units = sorted(ready, key=lambda u: (round(ready[u], 1), str(u)))
    return [(0, 0, 0), (1, 0, 0)] + units


UNITS = unit_order()
SLOT = {u: n for n, u in enumerate(UNITS)}
N_UNITS = len(UNITS) + 1
CTX_SLOT = len(UNITS)


def item_steps(per_step=0.62):
    steps = {}
    now = 0.0
    placed = set()
    plan = []
    for n in range(N_UNITS):
        need = []
        if n < len(UNITS):
            need = [k for k in ITEM_ORDER if k[:3] == UNITS[n] and k not in placed]
        for k in need:
            now = max(now, ARRIVE[k])
        early = [k for k in ITEM_ORDER if k not in placed and (k in need or ARRIVE[k] <= now)]
        placed.update(early)
        plan.append(early)
        now += per_step
    return plan


PLAN = item_steps()


class Board:
    def __init__(self, sends, recvs):
        self.sends, self.recvs, self.count, self.started = sends, recvs, 0, []

    def take(self, n=1):
        first = self.count
        self.count += n
        return first

    def send(self, number, src, dst, device):
        copy = pltpu.make_async_remote_copy(
            src_ref=src, dst_ref=dst, send_sem=self.sends.at[number],
            recv_sem=self.recvs.at[number], device_id=device,
            device_id_type=pl.DeviceIdType.MESH)
        copy.start()

    def arrived(self, number, dst, device):
        pltpu.make_async_remote_copy(
            src_ref=dst, dst_ref=dst, send_sem=self.sends.at[number],
            recv_sem=self.recvs.at[number], device_id=device,
            device_id_type=pl.DeviceIdType.MESH).wait_recv()

    def sent(self, number, src, device):
        pltpu.make_async_remote_copy(
            src_ref=src, dst_ref=src, send_sem=self.sends.at[number],
            recv_sem=self.recvs.at[number], device_id=device,
            device_id_type=pl.DeviceIdType.MESH).wait_send()


class Place:
    def __init__(self):
        self.s = lax.axis_index("sp")
        self.t = lax.axis_index("tp")
        self.y, self.x = self.s // 4, self.s % 4
        self.z, self.c = self.t // 2, self.t % 2

    def plane(self, axis, step):
        y, x = self.y, self.x
        if axis == "x":
            x = (x + step + 4) % 4
        else:
            y = (y + step + 4) % 4
        return {"sp": y * 4 + x, "tp": self.t}

    def sp_peer(self, k):
        return {"sp": (self.s + k) % 16, "tp": self.t}

    def tp_peer(self, k):
        return {"sp": self.s, "tp": (self.t + k) % 16}

    def ring(self, step):
        return {"sp": self.s, "tp": ((self.z + step + 8) % 8) * 2 + self.c}

    def sibling(self):
        return {"sp": self.s, "tp": self.z * 2 + 1 - self.c}


def greet(devices):
    barrier = pltpu.get_barrier_semaphore()
    for device in devices:
        pl.semaphore_signal(barrier, inc=1, device_id=device,
                            device_id_type=pl.DeviceIdType.MESH)
    pl.semaphore_wait(barrier, len(devices))


class ZRing:
    def __init__(self, board, place, own, bufs, by_device=False):
        self.board, self.place, self.own, self.bufs = board, place, own, bufs
        self.by_device = by_device
        self.base = board.take(16)

    def number(self, way, dist, part):
        return self.base + (0 if way == 1 else 8) + (dist - 1) * 2 + part

    def slot(self, way, dist, part):
        return self.bufs[part].at[self.index(way * dist)]

    def index(self, back):
        at = (self.place.z - back + 16) % 8
        return at * 2 + self.place.c if self.by_device else at

    def begin(self):
        for part in (0, 1):
            for way in (1, -1):
                self.board.send(self.number(way, 1, part), self.own[part],
                                self.bufs[part].at[self.index(0)], self.place.ring(way))

    def take(self, way, dist, part):
        here = self.slot(way, dist, part)
        self.board.arrived(self.number(way, dist, part), here, self.place.ring(-way))
        if dist < 3 or (dist == 3 and part == (0 if way == 1 else 1)):
            self.board.send(self.number(way, dist + 1, part), here, here, self.place.ring(way))

    def items(self):
        out = []
        for dist in (1, 2, 3):
            for part in (0, 1):
                for way in (1, -1):
                    out.append((way, dist, part))
        out.append((1, 4, 0))
        out.append((-1, 4, 1))
        return out

    def drain(self):
        for part in (0, 1):
            for way in (1, -1):
                self.board.sent(self.number(way, 1, part), self.own[part], self.place.ring(way))
        for way, dist, part in self.items():
            if dist > 1:
                here = self.slot(way, dist - 1, part)
                self.board.sent(self.number(way, dist, part), here, self.place.ring(way))


def quarter_ref(buf, slot, part):
    if part == "U":
        return buf.at[slot]
    return buf.at[slot, part]


def whole_kernel(lat_ref, context_ref, cond_ref, condc_ref, mw_ref, ng_ref, dq_ref, dkv_ref,
                 rw_ref, qlg_ref, kvlg_ref, upq_ref, upk_ref, upv_ref, qg_ref, kg_ref, bias_ref,
                 ow_ref, base_ref, tab_ref, out_ref,
                 wq, wkv, latsib, modp, modf, xn, uq, ukv, sq, skv, lq, lk, upt, wk, pad,
                 qt, kvb, cbuf, owa, owb, s_a, s_b, mb_a, mb_b, m_ref, l_ref, acc, att, attb,
                 part_ref, sib_ref, sends, recvs):
    place = Place()
    board = Board(sends, recvs)
    kv_base = board.take(len(ITEM_ORDER))
    ctx_base = board.take(16)
    a2a_base = board.take(8)
    d2d = board.take(1)
    lat_d2d = board.take(1)
    modp_base = board.take(16)
    modf_base = board.take(16)
    part_base = board.take(2)
    share_base = board.take(16)
    half_cols = D // 2
    ring = ZRing(board, place, (ow_ref.at[:, :half_cols], ow_ref.at[:, half_cols:]), (owa, owb))
    wring = ZRing(board, place, (dq_ref, dkv_ref), (wq, wkv))
    lring = ZRing(board, place, (lq.at[place.t], lk.at[place.t]), (lq, lk), by_device=True)

    greet([place.sp_peer(k) for k in range(1, 16)] + [place.tp_peer(k) for k in range(1, 16)])

    wring.begin()
    board.send(lat_d2d, lat_ref, latsib, place.sibling())

    span = pl.ds(pl.multiple_of(place.s * 128, 128), 128)

    def silu(v):
        v = v.astype(F32)
        return v / (1.0 + jnp.exp(-v))

    act = jnp.concatenate(
        [silu(cond_ref[:, span]), silu(condc_ref[:, span]), jnp.zeros((14, 128), F32)],
        axis=0).astype(BF)
    terms = [jnp.dot(act, mw_ref[r], preferred_element_type=F32) for r in range(3)]
    modp[place.s] = jnp.concatenate(
        [terms[0][0:1], terms[1][0:1], terms[2][0:1], terms[0][1:2], terms[1][1:2],
         jnp.zeros((3, 128), F32)], axis=0)
    for k in range(1, 16):
        board.send(modp_base + k, modp.at[place.s], modp.at[place.s], place.sp_peer(k))

    wq[place.z] = dq_ref[...]
    wkv[place.z] = dkv_ref[...]
    owa[place.z] = ow_ref[:, :half_cols]
    owb[place.z] = ow_ref[:, half_cols:]
    pad[...] = jnp.zeros(pad.shape, F32)
    pad[:, 0:HEAD] = upq_ref[...].astype(F32)
    upt[...] = pad[...].T.astype(BF)
    wk[...] = jnp.zeros(wk.shape, BF)
    pad[0:512, 0:NOPE] = upk_ref[...].astype(F32)
    pad[0:512, NOPE:128] = upv_ref[...].astype(F32)
    turned_up = pad[0:512, :].T.astype(BF)
    wk[0:NOPE, 0:512] = turned_up[0:NOPE]
    wk[HEAD:HEAD + VDIM, 0:512] = turned_up[NOPE:128]
    unit = (lax.broadcasted_iota(jnp.int32, (ROPE, 128), 0)
            == lax.broadcasted_iota(jnp.int32, (ROPE, 128), 1))
    wk[NOPE:HEAD, 512:640] = jnp.where(unit, 1.0, 0.0).astype(BF)

    def inverse(ref):
        rows = ref[...].astype(F32)
        return lax.rsqrt(jnp.mean(rows * rows, axis=-1, keepdims=True) + epsilon)

    inv_own = inverse(lat_ref)
    inv_ctx = inverse(context_ref)

    for k in range(1, 16):
        board.arrived(modp_base + k, modp.at[(place.s - k + 16) % 16], place.sp_peer(16 - k))
    modf[place.t] = jnp.sum(modp[...], axis=0)
    for k in range(1, 16):
        board.send(modf_base + k, modf.at[place.t], modf.at[place.t], place.tp_peer(k))

    board.arrived(lat_d2d, latsib, place.sibling())
    inv_sib = inverse(latsib)
    w_items = wring.items()
    for item in w_items[:4]:
        wring.take(*item)
    for k in range(1, 16):
        board.arrived(modf_base + k, modf.at[(place.t - k + 16) % 16], place.tp_peer(16 - k))

    for k in range(16):
        cols = slice(k * 128, (k + 1) * 128)
        gain = ng_ref[:, cols].astype(F32)
        shift, scale = modf[k, 0:1, :], modf[k, 1:2, :]
        own = lat_ref[:, cols].astype(F32) * inv_own * gain
        xn[k, 0:64] = (own * (1.0 + scale) + shift).astype(BF)
        sib = latsib[:, cols].astype(F32) * inv_sib * gain
        xn[k, 96:160] = (sib * (1.0 + scale) + shift).astype(BF)
        ctx = context_ref[:, cols].astype(F32) * inv_ctx * gain
        xn[k, 64:96] = (ctx * (1.0 + modf[k, 4:5, :]) + modf[k, 3:4, :]).astype(BF)

    def add_product(at, part):
        rows = xn[2 * at + place.c]
        if part == 0:
            uq[...] += jnp.dot(rows, wq[at], preferred_element_type=F32)
        else:
            ukv[...] += jnp.dot(rows, wkv[at], preferred_element_type=F32)

    uq[...] = jnp.dot(xn[place.t], wq[place.z], preferred_element_type=F32)
    ukv[...] = jnp.dot(xn[place.t], wkv[place.z], preferred_element_type=F32)
    rope = jnp.dot(xn[0, 0:96], rw_ref[0:128], preferred_element_type=F32)
    for k in range(1, 16):
        rope = rope + jnp.dot(xn[k, 0:96], rw_ref[k * 128:(k + 1) * 128],
                              preferred_element_type=F32)
    rope = rope.astype(BF).astype(F32)
    for n, (way, dist, part) in enumerate(w_items):
        if n >= 4:
            wring.take(way, dist, part)
        add_product(wring.index(way * dist), part)

    board.send(part_base, uq.at[96:160], sq, place.sibling())
    board.send(part_base + 1, ukv.at[64:160], skv, place.sibling())

    def latent_of(total, gain_ref):
        return (total * lax.rsqrt(jnp.mean(total * total, axis=-1, keepdims=True) + epsilon)
                * gain_ref[...].astype(F32)).astype(BF)

    board.arrived(part_base, sq, place.sibling())
    lq[place.t] = latent_of(uq[0:64] + sq[...], qlg_ref)
    board.arrived(part_base + 1, skv, place.sibling())
    lk[place.t, :, 0:512] = latent_of(ukv[0:64] + skv[32:96], kvlg_ref)
    lk[place.t, :, 512:640] = jnp.concatenate(
        [rope[0:64], jnp.zeros((64, 96), F32)], axis=1).astype(BF)
    lring.begin()

    def share(number, ref):
        board.send(share_base + number, ref, ref, place.sibling())

    share(0, lq.at[place.t])
    share(1, lk.at[place.t])

    ctx_kv = latent_of(ukv[64:96] + skv[0:32], kvlg_ref)
    ctx_k = jnp.dot(ctx_kv, upk_ref[...], preferred_element_type=F32)
    ctx_v = jnp.dot(ctx_kv, upv_ref[...], preferred_element_type=F32)
    ctx_u = jnp.concatenate([ctx_k, rope[64:96]], axis=1)
    ctx_n = ctx_u * lax.rsqrt(jnp.mean(ctx_u * ctx_u, axis=-1, keepdims=True) + epsilon)
    ctx_n = ctx_n * kg_ref[...]
    cbuf[place.s] = jnp.concatenate(
        [ctx_n, jnp.zeros((CTX_DEV, 128 - HEAD), F32), ctx_v,
         jnp.zeros((CTX_DEV, 128 - VDIM), F32)], axis=1).astype(BF)
    for k in range(1, 16):
        board.send(ctx_base + k, cbuf.at[place.s], cbuf.at[place.s], place.sp_peer(k))

    base = base_ref[pl.ds(pl.multiple_of(place.s * 16, 16), 16)]
    base_cos, base_sin = base[0:8, 0:1], base[8:16, 0:1]
    row_cos = tab_ref[0:8] * base_cos - tab_ref[8:16] * base_sin
    row_sin = tab_ref[8:16] * base_cos + tab_ref[0:8] * base_sin
    col_cos, col_sin = tab_ref[16:24], tab_ref[24:32]

    def column(gain_ref):
        row = jnp.concatenate([gain_ref[...], jnp.zeros((1, 128 - HEAD), F32)], axis=1)
        return jnp.broadcast_to(row, (128, 128)).T[0:HEAD, 0:1]

    def turned(u, gain):
        normal = u * lax.rsqrt(jnp.mean(u * u, axis=0, keepdims=True) + epsilon) * gain
        a, b, c, d = (normal[NOPE + 8 * n:NOPE + 8 * n + 8] for n in range(4))
        return jnp.concatenate(
            [normal[0:NOPE], a * row_cos - b * row_sin, b * row_cos + a * row_sin,
             c * col_cos - d * col_sin, d * col_cos + c * col_sin], axis=0)

    query_gain, key_gain = column(qg_ref), column(kg_ref)

    own_at = [(1, 0), (-1, 0)]
    for n, (way, dist, part) in enumerate(lring.items()):
        lring.take(way, dist, part)
        share(2 + n, lring.slot(way, dist, part))
    other = 1 - place.c
    for part, buf in enumerate((lq, lk)):
        board.arrived(share_base + part, buf.at[place.z * 2 + other], place.sibling())
    for n, (way, dist, part) in enumerate(lring.items()):
        at = ((place.z - way * dist + 16) % 8) * 2 + other
        board.arrived(share_base + 2 + n, (lq, lk)[part].at[at], place.sibling())

    contract = (((1,), (1,)), ((), ()))
    kv = lax.dot_general(wk[...], lk[...].reshape(1024, 640), contract,
                         preferred_element_type=F32)
    kv = jnp.concatenate([turned(kv[0:HEAD], key_gain), kv[HEAD:HEAD + VDIM]],
                         axis=0).astype(BF)
    for h in (0, 1):
        for q in (0, 1):
            at = (2 * h + q) * 256
            kvb[SLOT[(h, 0, 0)], q] = kv[:, at:at + 256]

    def queries():
        u = lax.dot_general(upt[...], lq[...].reshape(1024, 768), contract,
                            preferred_element_type=F32)
        qt[0:HEAD] = turned(u[0:HEAD], query_gain).astype(BF)
        qt[HEAD:128] = jnp.zeros((128 - HEAD, 1024), BF)

    def finish():
        wring.drain()
        lring.drain()
        board.sent(lat_d2d, lat_ref, place.sibling())
        for k in range(1, 16):
            board.sent(modp_base + k, modp.at[place.s], place.sp_peer(k))
            board.sent(modf_base + k, modf.at[place.t], place.tp_peer(k))
        board.sent(part_base, uq.at[96:160], place.sibling())
        board.sent(part_base + 1, ukv.at[64:160], place.sibling())
        share_sizes = [0, 1] + [item[2] for item in lring.items()]
        for n, part in enumerate(share_sizes):
            board.sent(share_base + n, (lq, lk)[part].at[0], place.sibling())

    def kv_send(key, src):
        axis, step, _ = ITEMS[key]
        h, da, db, part = key
        board.send(kv_base + ITEM_INDEX[key], src, quarter_ref(kvb, SLOT[key[:3]], part),
                   place.plane(axis, step))

    def own_part(h):
        return kvb.at[SLOT[(h, 0, 0)]]

    for key in sorted((k for k in ITEMS if ITEMS[k][2] is None),
                      key=lambda k: 0 if ITEMS[k][0] == ("x" if k[0] == 0 else "y") else 1):
        kv_send(key, own_part(key[0]))
    ring.begin()
    queries()

    def kv_take(key):
        axis, step, _ = ITEMS[key]
        here = quarter_ref(kvb, SLOT[key[:3]], key[3])
        board.arrived(kv_base + ITEM_INDEX[key], here, place.plane(axis, -step))
        for other in ITEM_ORDER:
            if ITEMS[other][2] == key:
                src = here
                if key[3] == "U" and other[3] != "U":
                    src = kvb.at[SLOT[key[:3]], other[3]]
                kv_send(other, src)

    def ctx_unit():
        for k in range(1, 16):
            board.arrived(ctx_base + k, cbuf.at[(place.s - k + 16) % 16], place.sp_peer(16 - k))
        turned = cbuf[...].reshape(512, 256).astype(F32).T.astype(BF)
        for q in (0, 1):
            kvb[CTX_SLOT, q, 0:HEAD, :] = turned[0:HEAD, q * 256:(q + 1) * 256]
            kvb[CTX_SLOT, q, HEAD:HEAD + VDIM, :] = turned[128:128 + VDIM, q * 256:(q + 1) * 256]

    m_ref[...] = jnp.full(m_ref.shape, -jnp.inf, F32)
    l_ref[...] = jnp.zeros(l_ref.shape, F32)
    acc[...] = jnp.zeros(acc.shape, F32)

    def products(slot, s_ref, mb_ref):
        for q in (0, 1):
            keys = kvb[slot, q, 0:128, :].T
            for n in range(4):
                cols = slice(n * 256, (n + 1) * 256)
                scores = jnp.dot(keys, qt[:, cols], preferred_element_type=F32)
                s_ref[q * 256:(q + 1) * 256, cols] = scores
                top = jnp.max(scores, axis=0, keepdims=True)
                mb_ref[:, cols] = top if q == 0 else jnp.maximum(mb_ref[:, cols], top)

    def absorb(slot, s_ref, mb_ref, bias):
        for n in range(4):
            cols = slice(n * 256, (n + 1) * 256)
            old = m_ref[:, cols]
            top = mb_ref[:, cols] * SCALE2
            if bias is not None:
                top = top + bias
            new = jnp.maximum(old, top)
            m_ref[:, cols] = new
            factor = jnp.exp2(old - new)
            less = new if bias is None else new - bias
            weights = jnp.exp2(s_ref[:, cols] * SCALE2 - less)
            l_ref[:, cols] = l_ref[:, cols] * factor + jnp.sum(weights, axis=0, keepdims=True)
            rounded = weights.astype(BF)
            summed = jnp.dot(kvb[slot, 0, HEAD:HEAD + VDIM, :], rounded[:256],
                             preferred_element_type=F32)
            summed = summed + jnp.dot(kvb[slot, 1, HEAD:HEAD + VDIM, :], rounded[256:],
                                      preferred_element_type=F32)
            acc[:, cols] = acc[:, cols] * factor + summed

    ring_items = ring.items()
    ring_plan = [[] for _ in range(N_UNITS)]
    for n, item in enumerate(ring_items):
        ring_plan[min(4 + (n * 26) // len(ring_items), N_UNITS - 1)].append(item)

    def actions(n):
        for key in PLAN[n]:
            kv_take(key)
        for item in ring_plan[n]:
            ring.take(*item)
        if n == CTX_SLOT:
            ctx_unit()

    def act_in_loop(i, offset):
        for trip in range(16):
            n = 2 * trip + offset
            if PLAN[n] or ring_plan[n] or n == CTX_SLOT:
                @pl.when(i == trip)
                def _():
                    actions(n)

    actions(0)
    products(0, s_a, mb_a)

    def body(i, carry):
        act_in_loop(i, 1)
        products(2 * i + 1, s_b, mb_b)
        absorb(2 * i, s_a, mb_a, None)
        act_in_loop(i, 2)
        products(2 * i + 2, s_a, mb_a)
        absorb(2 * i + 1, s_b, mb_b, None)
        return carry

    lax.fori_loop(0, 16, body, 0)
    bias = (bias_ref[0, 0] + math.log(TOK_DEV / CTX_DEV)) * LOG2E
    absorb(CTX_SLOT, s_a, mb_a, bias)

    for k in range(8):
        cols = slice(k * 128, (k + 1) * 128)
        att[k] = (acc[:, cols] / l_ref[:, cols]).astype(BF)
    for k in range(1, 8):
        board.send(a2a_base + k, att.at[(place.z + k) % 8], attb.at[place.z], place.ring(k))
    attb[place.z] = att[place.z]
    for k in range(1, 8):
        board.arrived(a2a_base + k, attb.at[(place.z - k + 8) % 8], place.ring(-k))
    rows = attb[...].reshape(8 * VDIM, 128).astype(F32).T.astype(BF)
    for n, weight in enumerate((owa, owb)):
        part_ref[:, n * half_cols:(n + 1) * half_cols] = jnp.dot(
            rows, weight[...].reshape(8 * VDIM, half_cols), preferred_element_type=F32)
    away = part_ref.at[pl.ds(pl.multiple_of(64 * (1 - place.c), 64), 64)]
    board.send(d2d, away, sib_ref, place.sibling())
    board.arrived(d2d, sib_ref, place.sibling())
    gates = jnp.concatenate([modf[k, 2:3, :] for k in range(16)], axis=1)
    mine = part_ref[pl.ds(pl.multiple_of(64 * place.c, 64), 64)]
    projected = mine + sib_ref[...]
    out_ref[...] = (lat_ref[...].astype(F32) + gates * projected).astype(BF)

    board.sent(d2d, away, place.sibling())
    for k in range(1, 8):
        board.sent(a2a_base + k, att.at[(place.z + k) % 8], place.ring(k))
    for k in range(1, 16):
        board.sent(ctx_base + k, cbuf.at[place.s], place.sp_peer(k))
    ring.drain()
    finish()
    for key in ITEM_ORDER:
        axis, step, _ = ITEMS[key]
        src = quarter_ref(kvb, 0, key[3])
        board.sent(kv_base + ITEM_INDEX[key], src, place.plane(axis, step))


def rotation_tables():
    frequency = np.power(np.float32(theta), -np.arange(8, dtype=np.float32) / np.float32(8))
    frequency = frequency.astype(np.float32).astype(np.float64)[:, None]
    token = np.arange(1024)[None, :]
    row, col = frequency * (token // GRID_W), frequency * (token % GRID_W)
    table = np.concatenate([np.cos(row), np.sin(row), np.cos(col), np.sin(col)])
    first = frequency * (np.arange(16)[None, :] * 16)
    base = np.stack([np.cos(first), np.sin(first)]).reshape(16, 16).T.reshape(256, 1)
    base = np.broadcast_to(base, (256, 128))
    return base.astype(np.float32), table.astype(np.float32)


def shards(
    latent,
    context,
    cond,
    cond_context,
    mod_weight,
    norm_gain,
    down_q,
    down_kv,
    rope_weight,
    qlat_gain,
    kvlat_gain,
    up_query,
    up_key,
    up_value,
    query_gain,
    key_gain,
    context_bias,
    out_weight,
):
    vmem = pl.BlockSpec(memory_space=pltpu.VMEM)
    smem = pl.BlockSpec(memory_space=pltpu.SMEM)
    copies = len(ITEM_ORDER) + 16 + 8 + 2 + 32 + 2 + 16 + 3 * 16
    base, table = rotation_tables()
    row = lambda v: v.reshape(1, -1)
    return pl.pallas_call(
        whole_kernel,
        out_shape=jax.ShapeDtypeStruct((64, D), BF),
        in_specs=[vmem] * 16 + [smem] + [vmem] * 3,
        out_specs=vmem,
        scratch_shapes=[
            pltpu.VMEM((8, 128, 768), BF),
            pltpu.VMEM((8, 128, 512), BF),
            pltpu.VMEM((64, D), BF),
            pltpu.VMEM((16, 8, 128), F32),
            pltpu.VMEM((16, 8, 128), F32),
            pltpu.VMEM((16, 160, 128), BF),
            pltpu.VMEM((160, 768), F32),
            pltpu.VMEM((160, 512), F32),
            pltpu.VMEM((64, 768), F32),
            pltpu.VMEM((96, 512), F32),
            pltpu.VMEM((16, 64, 768), BF),
            pltpu.VMEM((16, 64, 640), BF),
            pltpu.VMEM((128, 768), BF),
            pltpu.VMEM((160, 640), BF),
            pltpu.VMEM((768, 128), F32),
            pltpu.VMEM((128, 1024), BF),
            pltpu.VMEM((N_UNITS, 2, HEAD + VDIM, 256), BF),
            pltpu.VMEM((16, CTX_DEV, 256), BF),
            pltpu.VMEM((8, 64, D // 2), BF),
            pltpu.VMEM((8, 64, D // 2), BF),
            pltpu.VMEM((512, 1024), F32),
            pltpu.VMEM((512, 1024), F32),
            pltpu.VMEM((1, 1024), F32),
            pltpu.VMEM((1, 1024), F32),
            pltpu.VMEM((1, 1024), F32),
            pltpu.VMEM((1, 1024), F32),
            pltpu.VMEM((VDIM, 1024), F32),
            pltpu.VMEM((8, VDIM, 128), BF),
            pltpu.VMEM((8, VDIM, 128), BF),
            pltpu.VMEM((128, D), F32),
            pltpu.VMEM((64, D), F32),
            pltpu.SemaphoreType.DMA((copies,)),
            pltpu.SemaphoreType.DMA((copies,)),
        ],
        compiler_params=pltpu.CompilerParams(collective_id=0, has_side_effects=True,
                                             vmem_limit_bytes=56 * 1024 * 1024),
        name="whole",
    )(latent, context, row(cond), row(cond_context), mod_weight, row(norm_gain), down_q, down_kv,
      rope_weight, row(qlat_gain), row(kvlat_gain), up_query, up_key, up_value, row(query_gain),
      row(key_gain), context_bias.reshape(1, 1), out_weight, jnp.asarray(base),
      jnp.asarray(table))


def solution(mesh):
    placed = (
        P(SP_TP, None),
        P("sp", None),
        P(),
        P(),
        P(None, "sp", "tp"),
        P(),
        P("tp", None),
        P("tp", None),
        P(),
        P(),
        P(),
        P(None, "tp"),
        P(None, "tp"),
        P(None, "tp"),
        P(),
        P(),
        P("tp"),
        P("tp", None),
    )
    return jax.shard_map(
        shards, mesh=mesh, in_specs=placed, out_specs=P(SP_TP, None), check_vma=False
    )
```

```python
import math

import jax
import jax.numpy as jnp
import numpy as np
from jax import lax
from jax.experimental import pallas as pl
from jax.experimental.pallas import tpu as pltpu
from jax.sharding import PartitionSpec as P

NOPE = 64
ROPE = 32
HEAD = NOPE + ROPE
VDIM = 64
GRID_W = 64
TOK_DEV = 1024
CTX_DEV = 32
D = 2048
SP_TP = ("sp", "tp")
BF = jnp.bfloat16
F32 = jnp.float32

epsilon = 1e-06
theta = 10000.0
SCALE2 = math.log2(math.e) * HEAD ** (-0.5)
LOG2E = math.log2(math.e)


def exchange_items():
    items = {}
    for h in (0, 1):
        def add(da, db, part, axis, step, trigger):
            names = ("x", "y") if h == 0 else ("y", "x")
            items[(h, da, db, part)] = (names[axis], step, trigger)
        add(-1, 0, "U", 0, 1, None)
        add(1, 0, "U", 0, -1, None)
        add(2, 0, 0, 0, 1, (h, -1, 0, "U"))
        add(2, 0, 1, 0, -1, (h, 1, 0, "U"))
        for da in (0, -1, 1):
            trigger = None if da == 0 else (h, da, 0, "U")
            add(da, -1, "U", 1, 1, trigger)
            add(da, 1, "U", 1, -1, trigger)
            add(da, 2, 0, 1, 1, (h, da, -1, "U"))
            add(da, 2, 1, 1, -1, (h, da, 1, "U"))
        for q in (0, 1):
            add(2, -1, q, 1, 1, (h, 2, 0, q))
            add(2, 1, q, 1, -1, (h, 2, 0, q))
        add(2, 2, 0, 1, 1, (h, 2, -1, 0))
        add(2, 2, 1, 1, -1, (h, 2, 1, 1))
    return items


RELEASE = (10.0, 17.5)
EARLY_AT = 16.0
LOOP_AT = 19.5
STEP = 0.78
UNIT, LATENCY = 3.53, 1.9


def plan_exchange(items):
    free, arrive = {}, {}
    left = dict(items)

    def send(key, at):
        axis, step, _ = items[key]
        begin = max(at, free.get((axis, step), 0.0))
        free[(axis, step)] = begin + (UNIT if key[3] == "U" else UNIT / 2)
        arrive[key] = free[(axis, step)] + LATENCY

    def begin_half(h, at):
        keys = [k for k in items if items[k][2] is None and k[0] == h]
        first = "x" if h == 0 else "y"
        for key in sorted(keys, key=lambda k: 0 if items[k][0] == first else 1):
            send(key, at)

    taken = []

    def rank(key):
        return (round(arrive[key], 1), 0 if key[2] == 0 else 1, str(key))

    def take(now, limit=None):
        got = []
        while True:
            here = sorted((k for k in arrive if k not in taken and arrive[k] <= now), key=rank)
            if not here or (limit is not None and len(got) >= limit):
                return got
            key = here[0]
            taken.append(key)
            got.append(key)
            for other in items:
                if items[other][2] == key:
                    send(other, now)

    begin_half(0, RELEASE[0])
    early = take(EARLY_AT, 3)
    begin_half(1, RELEASE[1])
    now = LOOP_AT
    units = [(0, 0, 0), (1, 0, 0)]
    every = sorted({k[:3] for k in items})

    def ready():
        done = [u for u in every if u not in units
                and all(k in taken for k in items if k[:3] == u)]
        return sorted(done, key=lambda u: (max(arrive[k] for k in items if k[:3] == u), str(u)))

    plan = [take(now)]
    for n in range(1, len(every) + 3, 2):
        got = take(now)
        while len(units) < min(n + 2, len(every) + 2):
            come = ready()
            if come:
                units.append(come[0])
                continue
            now = min(arrive[k] for k in arrive if k not in taken)
            got = got + take(now)
        plan.append(got)
        now += 2 * STEP
    return early, plan, units, now


ITEMS = exchange_items()
EARLY, PLAN, UNITS, PLAN_END = plan_exchange(ITEMS)
ITEM_ORDER = list(ITEMS)
ITEM_INDEX = {k: n for n, k in enumerate(ITEM_ORDER)}
SLOT = {u: n for n, u in enumerate(UNITS)}
N_UNITS = len(UNITS) + 1
CTX_SLOT = len(UNITS)


def mark(name):
    pass


class Board:
    def __init__(self, sends, recvs):
        self.sends, self.recvs, self.count, self.started = sends, recvs, 0, []

    def take(self, n=1):
        first = self.count
        self.count += n
        return first

    def send(self, number, src, dst, device):
        copy = pltpu.make_async_remote_copy(
            src_ref=src, dst_ref=dst, send_sem=self.sends.at[number],
            recv_sem=self.recvs.at[number], device_id=device,
            device_id_type=pl.DeviceIdType.MESH)
        copy.start()

    def arrived(self, number, dst, device):
        pltpu.make_async_remote_copy(
            src_ref=dst, dst_ref=dst, send_sem=self.sends.at[number],
            recv_sem=self.recvs.at[number], device_id=device,
            device_id_type=pl.DeviceIdType.MESH).wait_recv()

    def sent(self, number, src, device):
        pltpu.make_async_remote_copy(
            src_ref=src, dst_ref=src, send_sem=self.sends.at[number],
            recv_sem=self.recvs.at[number], device_id=device,
            device_id_type=pl.DeviceIdType.MESH).wait_send()


class Place:
    def __init__(self):
        self.s = lax.axis_index("sp")
        self.t = lax.axis_index("tp")
        self.y, self.x = self.s // 4, self.s % 4
        self.z, self.c = self.t // 2, self.t % 2

    def plane(self, axis, step):
        y, x = self.y, self.x
        if axis == "x":
            x = (x + step + 4) % 4
        else:
            y = (y + step + 4) % 4
        return {"sp": y * 4 + x, "tp": self.t}

    def sp_peer(self, k):
        return {"sp": (self.s + k) % 16, "tp": self.t}

    def tp_peer(self, k):
        return {"sp": self.s, "tp": (self.t + k) % 16}

    def ring(self, step):
        return {"sp": self.s, "tp": ((self.z + step + 8) % 8) * 2 + self.c}

    def sibling(self):
        return {"sp": self.s, "tp": self.z * 2 + 1 - self.c}


def greet(devices):
    barrier = pltpu.get_barrier_semaphore()
    for device in devices:
        pl.semaphore_signal(barrier, inc=1, device_id=device,
                            device_id_type=pl.DeviceIdType.MESH)
    pl.semaphore_wait(barrier, len(devices))


class ZRing:
    def __init__(self, board, place, own, bufs, by_device=False):
        self.board, self.place, self.own, self.bufs = board, place, own, bufs
        self.by_device = by_device
        self.base = board.take(16)

    def number(self, way, dist, part):
        return self.base + (0 if way == 1 else 8) + (dist - 1) * 2 + part

    def slot(self, way, dist, part):
        return self.bufs[part].at[self.index(way * dist)]

    def index(self, back):
        at = (self.place.z - back + 16) % 8
        return at * 2 + self.place.c if self.by_device else at

    def begin(self):
        for part in (0, 1):
            self.begin_part(part)

    def begin_part(self, part):
        for way in (1, -1):
            self.board.send(self.number(way, 1, part), self.own[part],
                            self.bufs[part].at[self.index(0)], self.place.ring(way))

    def take(self, way, dist, part):
        here = self.slot(way, dist, part)
        self.board.arrived(self.number(way, dist, part), here, self.place.ring(-way))
        if dist < 3 or (dist == 3 and part == (0 if way == 1 else 1)):
            self.board.send(self.number(way, dist + 1, part), here, here, self.place.ring(way))

    def items(self):
        out = []
        for dist in (1, 2, 3):
            for part in (0, 1):
                for way in (1, -1):
                    out.append((way, dist, part))
        out.append((1, 4, 0))
        out.append((-1, 4, 1))
        return out

    def drain(self):
        for part in (0, 1):
            for way in (1, -1):
                self.board.sent(self.number(way, 1, part), self.own[part], self.place.ring(way))
        for way, dist, part in self.items():
            if dist > 1:
                here = self.slot(way, dist - 1, part)
                self.board.sent(self.number(way, dist, part), here, self.place.ring(way))


def quarter_ref(buf, slot, part):
    if part == "U":
        return buf.at[slot]
    return buf.at[slot, part]


def whole_kernel(lat_ref, context_ref, cond_ref, condc_ref, mw_ref, ng_ref, dq_ref, dkv_ref,
                 rw_ref, qlg_ref, kvlg_ref, upq_ref, upk_ref, upv_ref, qg_ref, kg_ref, bias_ref,
                 ow_ref, base_ref, tab_ref, out_ref,
                 wq, wkv, latsib, modp, modf, xn, uq, ukv, sq, skv, lq, lk, wk, rt,
                 qt, kvb, cbuf, owa, owb, s_a, s_b, mb_a, mb_b, m_ref, l_ref, acc, att, attb,
                 part_ref, sib_ref, sends, recvs):
    place = Place()
    board = Board(sends, recvs)
    kv_base = board.take(len(ITEM_ORDER))
    ctx_base = board.take(16)
    a2a_base = board.take(8)
    d2d = board.take(1)
    lat_d2d = board.take(1)
    modp_base = board.take(16)
    modf_base = board.take(16)
    part_base = board.take(2)
    share_base = board.take(16)
    half_cols = D // 2
    ring = ZRing(board, place, (ow_ref.at[:, :half_cols], ow_ref.at[:, half_cols:]), (owa, owb))
    wring = ZRing(board, place, (dq_ref, dkv_ref), (wq, wkv))
    lring = ZRing(board, place, (lk.at[place.t], lq.at[place.t]), (lk, lq), by_device=True)

    mark("a_greet")
    greet([place.sp_peer(k) for k in range(1, 16)] + [place.tp_peer(k) for k in range(1, 16)])

    mark("b_mod")
    wring.begin()
    board.send(lat_d2d, lat_ref, latsib, place.sibling())

    def silu(ref):
        rows = lax.broadcasted_iota(jnp.int32, (16, 128), 0)
        v = jnp.sum(jnp.where(rows == place.s, ref[...].astype(F32), 0.0), axis=0, keepdims=True)
        return v / (1.0 + jnp.exp(-v))

    act = jnp.concatenate(
        [silu(cond_ref), silu(condc_ref), jnp.zeros((14, 128), F32)],
        axis=0).astype(BF)
    terms = [jnp.dot(act, mw_ref[r], preferred_element_type=F32) for r in range(3)]
    modp[place.s] = jnp.concatenate(
        [terms[0][0:1], terms[1][0:1], terms[2][0:1], terms[0][1:2], terms[1][1:2],
         jnp.zeros((3, 128), F32)], axis=0)
    for k in range(1, 16):
        board.send(modp_base + k, modp.at[place.s], modp.at[place.s], place.sp_peer(k))

    mark("c_local")
    wq[place.z] = dq_ref[...]
    wkv[place.z] = dkv_ref[...]
    owa[place.z] = ow_ref[:, :half_cols]
    owb[place.z] = ow_ref[:, half_cols:]
    wk[...] = jnp.zeros(wk.shape, BF)
    wk[0:NOPE, 0:512] = upk_ref[...]
    wk[HEAD:HEAD + VDIM, 0:512] = upv_ref[...]
    unit = (lax.broadcasted_iota(jnp.int32, (ROPE, 128), 0)
            == lax.broadcasted_iota(jnp.int32, (ROPE, 128), 1))
    wk[NOPE:HEAD, 512:640] = jnp.where(unit, 1.0, 0.0).astype(BF)

    def inverse(ref):
        rows = ref[...].astype(F32)
        return lax.rsqrt(jnp.mean(rows * rows, axis=-1, keepdims=True) + epsilon)

    inv_own = inverse(lat_ref)
    inv_ctx = inverse(context_ref)

    mark("d_modwait")
    for k in range(1, 16):
        board.arrived(modp_base + k, modp.at[(place.s - k + 16) % 16], place.sp_peer(16 - k))
    modf[place.t] = jnp.sum(modp[...], axis=0)
    for k in range(1, 16):
        board.send(modf_base + k, modf.at[place.t], modf.at[place.t], place.tp_peer(k))

    board.arrived(lat_d2d, latsib, place.sibling())
    inv_sib = inverse(latsib)
    w_items = wring.items()
    for item in w_items[:4]:
        wring.take(*item)
    mark("e_modfwait")
    for k in range(1, 16):
        board.arrived(modf_base + k, modf.at[(place.t - k + 16) % 16], place.tp_peer(16 - k))

    mark("f_norm")
    norm_gain = ng_ref[...].astype(F32)
    for k in range(16):
        cols = slice(k * 128, (k + 1) * 128)
        gain = norm_gain[k:k + 1]
        shift, scale = modf[k, 0:1, :], modf[k, 1:2, :]
        own = lat_ref[:, cols].astype(F32) * inv_own * gain
        xn[k, 0:64] = (own * (1.0 + scale) + shift).astype(BF)
        sib = latsib[:, cols].astype(F32) * inv_sib * gain
        xn[k, 96:160] = (sib * (1.0 + scale) + shift).astype(BF)
        ctx = context_ref[:, cols].astype(F32) * inv_ctx * gain
        xn[k, 64:96] = (ctx * (1.0 + modf[k, 4:5, :]) + modf[k, 3:4, :]).astype(BF)

    def add_product(at, part):
        rows = xn[2 * at + place.c]
        if part == 0:
            uq[...] += jnp.dot(rows, wq[at], preferred_element_type=F32)
        else:
            ukv[...] += jnp.dot(rows, wkv[at], preferred_element_type=F32)

    uq[...] = jnp.dot(xn[place.t], wq[place.z], preferred_element_type=F32)
    ukv[...] = jnp.dot(xn[place.t], wkv[place.z], preferred_element_type=F32)
    contract = (((1,), (1,)), ((), ()))
    rope = jnp.zeros((96, ROPE), F32)
    for k in range(16):
        rope = rope + lax.dot_general(xn[k, 0:96], rw_ref[:, k * 128:(k + 1) * 128], contract,
                                      preferred_element_type=F32)
    rope = rope.astype(BF).astype(F32)
    mark("g_wring")
    for n, (way, dist, part) in enumerate(w_items):
        if n >= 4:
            wring.take(way, dist, part)
        add_product(wring.index(way * dist), part)

    mark("h_d2dpart")
    board.send(part_base + 1, ukv.at[64:160], skv, place.sibling())
    board.send(part_base, uq.at[96:160], sq, place.sibling())

    def latent_of(total, gain_ref):
        gain = gain_ref[...].astype(F32)
        gain = jnp.concatenate([gain[k:k + 1] for k in range(gain.shape[0])], axis=1)
        return (total * lax.rsqrt(jnp.mean(total * total, axis=-1, keepdims=True) + epsilon)
                * gain).astype(BF)

    board.arrived(part_base + 1, skv, place.sibling())
    lk[place.t, :, 0:512] = latent_of(ukv[0:64] + skv[32:96], kvlg_ref)
    lk[place.t, :, 512:640] = jnp.concatenate(
        [rope[0:64], jnp.zeros((64, 96), F32)], axis=1).astype(BF)
    def share(number, ref):
        board.send(share_base + number, ref, ref, place.sibling())

    lring.begin_part(0)
    share(0, lk.at[place.t])
    board.arrived(part_base, sq, place.sibling())
    lq[place.t] = latent_of(uq[0:64] + sq[...], qlg_ref)
    lring.begin_part(1)
    share(1, lq.at[place.t])

    mark("i_ctx")
    ctx_kv = latent_of(ukv[64:96] + skv[0:32], kvlg_ref)
    ctx_k = lax.dot_general(ctx_kv, upk_ref[...], contract, preferred_element_type=F32)
    ctx_v = lax.dot_general(ctx_kv, upv_ref[...], contract, preferred_element_type=F32)
    ctx_u = jnp.concatenate([ctx_k, rope[64:96]], axis=1)
    ctx_n = ctx_u * lax.rsqrt(jnp.mean(ctx_u * ctx_u, axis=-1, keepdims=True) + epsilon)
    ctx_n = ctx_n * kg_ref[...]
    cbuf[place.s] = jnp.concatenate(
        [ctx_n, jnp.zeros((CTX_DEV, 128 - HEAD), F32), ctx_v,
         jnp.zeros((CTX_DEV, 128 - VDIM), F32)], axis=1).astype(BF)
    for k in range(1, 16):
        board.send(ctx_base + k, cbuf.at[place.s], cbuf.at[place.s], place.sp_peer(k))

    base = base_ref[pl.ds(pl.multiple_of(place.s * 16, 16), 16)]
    base_cos, base_sin = base[0:8, 0:1], base[8:16, 0:1]
    rt[0:8] = tab_ref[0:8] * base_cos - tab_ref[8:16] * base_sin
    rt[8:16] = tab_ref[8:16] * base_cos + tab_ref[0:8] * base_sin
    rt[16:32] = tab_ref[16:32]

    def column(gain_ref):
        row = jnp.concatenate([gain_ref[...], jnp.zeros((1, 128 - HEAD), F32)], axis=1)
        return jnp.broadcast_to(row, (128, 128)).T[0:HEAD, 0:1]

    def turned(u, gain, cols):
        row_cos, row_sin = rt[0:8, cols], rt[8:16, cols]
        col_cos, col_sin = rt[16:24, cols], rt[24:32, cols]
        normal = u * lax.rsqrt(jnp.mean(u * u, axis=0, keepdims=True) + epsilon) * gain
        a, b, c, d = (normal[NOPE + 8 * n:NOPE + 8 * n + 8] for n in range(4))
        return jnp.concatenate(
            [normal[0:NOPE], a * row_cos - b * row_sin, b * row_cos + a * row_sin,
             c * col_cos - d * col_sin, d * col_cos + c * col_sin], axis=0)

    query_gain, key_gain = column(qg_ref), column(kg_ref)

    def finish():
        wring.drain()
        lring.drain()
        board.sent(lat_d2d, lat_ref, place.sibling())
        for k in range(1, 16):
            board.sent(modp_base + k, modp.at[place.s], place.sp_peer(k))
            board.sent(modf_base + k, modf.at[place.t], place.tp_peer(k))
        board.sent(part_base, uq.at[96:160], place.sibling())
        board.sent(part_base + 1, ukv.at[64:160], place.sibling())
        share_sizes = [0, 1] + [item[2] for item in l_items]
        for n, part in enumerate(share_sizes):
            board.sent(share_base + n, (lk, lq)[part].at[0], place.sibling())

    def kv_send(key, src):
        axis, step, _ = ITEMS[key]
        h, da, db, part = key
        board.send(kv_base + ITEM_INDEX[key], src, quarter_ref(kvb, SLOT[key[:3]], part),
                   place.plane(axis, step))

    def own_part(h):
        return kvb.at[SLOT[(h, 0, 0)]]

    def kv_begin(h):
        for key in sorted((k for k in ITEMS if ITEMS[k][2] is None and k[0] == h),
                          key=lambda k: 0 if ITEMS[k][0] == ("x" if k[0] == 0 else "y") else 1):
            kv_send(key, own_part(h))

    def kv_take(key):
        axis, step, _ = ITEMS[key]
        here = quarter_ref(kvb, SLOT[key[:3]], key[3])
        board.arrived(kv_base + ITEM_INDEX[key], here, place.plane(axis, -step))
        for other in ITEM_ORDER:
            if ITEMS[other][2] == key:
                src = here
                if key[3] == "U" and other[3] != "U":
                    src = kvb.at[SLOT[key[:3]], other[3]]
                kv_send(other, src)

    mark("j_lring")
    l_items = lring.items()
    other = 1 - place.c

    def ring_take(way, dist, part):
        lring.take(way, dist, part)
        share(2 + l_items.index((way, dist, part)), lring.slot(way, dist, part))

    def chip(dist, part):
        at = (place.z - dist + 16) % 8
        if dist == 0:
            number = part
        elif dist == 4:
            number = 2 + l_items.index((1 if part == 0 else -1, 4, part))
        else:
            number = 2 + l_items.index((1 if dist > 0 else -1, abs(dist), part))
        buf = (lk, lq)[part]
        board.arrived(share_base + number, buf.at[at * 2 + other], place.sibling())
        cols = pl.ds(pl.multiple_of(at * 128, 128), 128)
        return buf[pl.ds(at * 2, 2)].reshape(128, buf.shape[2]), cols

    def chip_keys(dist, h, n):
        rows, cols = chip(dist, 0)
        kv = lax.dot_general(wk[...], rows, contract, preferred_element_type=F32)
        kv = jnp.concatenate([turned(kv[0:HEAD], key_gain, cols), kv[HEAD:HEAD + VDIM]], axis=0)
        kvb[SLOT[(h, 0, 0)], n // 2, :, (n % 2) * 128:(n % 2) * 128 + 128] = kv.astype(BF)

    def chip_queries(dist):
        rows, cols = chip(dist, 1)
        u = lax.dot_general(upq_ref[...], rows, contract, preferred_element_type=F32)
        qt[0:HEAD, cols] = turned(u, query_gain, cols).astype(BF)

    qt[HEAD:128] = jnp.zeros((128 - HEAD, 1024), BF)
    ring_take(1, 1, 0)
    ring_take(-1, 1, 0)
    chip_keys(0, 0, 0)
    ring_take(1, 1, 1)
    ring_take(-1, 1, 1)
    chip_keys(1, 0, 1)
    chip_keys(-1, 0, 2)
    ring_take(1, 2, 0)
    ring_take(-1, 2, 0)
    chip_queries(0)
    chip_keys(2, 0, 3)
    mark("k_h0")
    kv_begin(0)
    ring_take(1, 2, 1)
    ring_take(-1, 2, 1)
    chip_queries(1)
    chip_queries(-1)
    ring_take(1, 3, 0)
    ring_take(-1, 3, 0)
    chip_keys(-2, 1, 0)
    chip_queries(2)
    ring_take(1, 3, 1)
    ring_take(-1, 3, 1)
    ring.begin()
    chip_keys(3, 1, 1)
    chip_keys(-3, 1, 2)
    chip_queries(-2)
    mark("l_early")
    for key in EARLY:
        kv_take(key)
    mark("l_h1")
    ring_take(1, 4, 0)
    chip_keys(4, 1, 3)
    kv_begin(1)
    mark("l_q")
    chip_queries(3)
    chip_queries(-3)
    ring_take(-1, 4, 1)
    chip_queries(4)

    def ctx_unit():
        for k in range(1, 16):
            board.arrived(ctx_base + k, cbuf.at[(place.s - k + 16) % 16], place.sp_peer(16 - k))
        turned = cbuf[...].reshape(512, 256).astype(F32).T.astype(BF)
        for q in (0, 1):
            kvb[CTX_SLOT, q, 0:HEAD, :] = turned[0:HEAD, q * 256:(q + 1) * 256]
            kvb[CTX_SLOT, q, HEAD:HEAD + VDIM, :] = turned[128:128 + VDIM, q * 256:(q + 1) * 256]

    mark("m_init")
    m_ref[...] = jnp.full(m_ref.shape, -jnp.inf, F32)
    l_ref[...] = jnp.zeros(l_ref.shape, F32)
    acc[...] = jnp.zeros(acc.shape, F32)

    def products(slot, s_ref, mb_ref):
        for q in (0, 1):
            keys = kvb[slot, q, 0:128, :].T
            for n in range(4):
                cols = slice(n * 256, (n + 1) * 256)
                scores = jnp.dot(keys, qt[:, cols], preferred_element_type=F32)
                s_ref[q * 256:(q + 1) * 256, cols] = scores
                top = jnp.max(scores, axis=0, keepdims=True)
                mb_ref[:, cols] = top if q == 0 else jnp.maximum(mb_ref[:, cols], top)

    def absorb(slot, s_ref, mb_ref, bias):
        for n in range(4):
            cols = slice(n * 256, (n + 1) * 256)
            old = m_ref[:, cols]
            top = mb_ref[:, cols] * SCALE2
            if bias is not None:
                top = top + bias
            new = jnp.maximum(old, top)
            m_ref[:, cols] = new
            factor = jnp.exp2(old - new)
            less = new if bias is None else new - bias
            weights = jnp.exp2(s_ref[:, cols] * SCALE2 - less)
            l_ref[:, cols] = l_ref[:, cols] * factor + jnp.sum(weights, axis=0, keepdims=True)
            rounded = weights.astype(BF)
            summed = jnp.dot(kvb[slot, 0, HEAD:HEAD + VDIM, :], rounded[:256],
                             preferred_element_type=F32)
            summed = summed + jnp.dot(kvb[slot, 1, HEAD:HEAD + VDIM, :], rounded[256:],
                                      preferred_element_type=F32)
            acc[:, cols] = acc[:, cols] * factor + summed

    ring_items = ring.items()
    ring_plan = [[] for _ in range(17)]
    for n, item in enumerate(ring_items):
        ring_plan[min(2 + (n * 13) // len(ring_items), 16)].append(item)

    def actions(n):
        for key in PLAN[n]:
            kv_take(key)
        for item in ring_plan[n]:
            ring.take(*item)

    mark("n_prolog")
    actions(0)
    products(0, s_a, mb_a)
    for i in range(16):
        mark(f"o{i:02d}a")
        actions(i + 1)
        if i == 15:
            ctx_unit()
        mark(f"o{i:02d}b")
        products(2 * i + 1, s_b, mb_b)
        absorb(2 * i, s_a, mb_a, None)
        products(2 * i + 2, s_a, mb_a)
        absorb(2 * i + 1, s_b, mb_b, None)
    mark("p_last")
    bias = (bias_ref[0, 0] + math.log(TOK_DEV / CTX_DEV)) * LOG2E
    absorb(CTX_SLOT, s_a, mb_a, bias)

    mark("q_a2a")
    for k in range(8):
        cols = slice(k * 128, (k + 1) * 128)
        att[k] = (acc[:, cols] / l_ref[:, cols]).astype(BF)
    for k in range(1, 8):
        board.send(a2a_base + k, att.at[(place.z + k) % 8], attb.at[place.z], place.ring(k))
    attb[place.z] = att[place.z]
    for k in range(1, 8):
        board.arrived(a2a_base + k, attb.at[(place.z - k + 8) % 8], place.ring(-k))
    mark("r_out")
    rows = attb[...].reshape(8 * VDIM, 128).astype(F32).T.astype(BF)
    for n, weight in enumerate((owa, owb)):
        part_ref[:, n * half_cols:(n + 1) * half_cols] = jnp.dot(
            rows, weight[...].reshape(8 * VDIM, half_cols), preferred_element_type=F32)
    away = part_ref.at[pl.ds(pl.multiple_of(64 * (1 - place.c), 64), 64)]
    mark("s_d2d")
    board.send(d2d, away, sib_ref, place.sibling())
    board.arrived(d2d, sib_ref, place.sibling())
    gates = jnp.concatenate([modf[k, 2:3, :] for k in range(16)], axis=1)
    mine = part_ref[pl.ds(pl.multiple_of(64 * place.c, 64), 64)]
    projected = mine + sib_ref[...]
    out_ref[...] = (lat_ref[...].astype(F32) + gates * projected).astype(BF)

    mark("t_drain")
    board.sent(d2d, away, place.sibling())
    for k in range(1, 8):
        board.sent(a2a_base + k, att.at[(place.z + k) % 8], place.ring(k))
    for k in range(1, 16):
        board.sent(ctx_base + k, cbuf.at[place.s], place.sp_peer(k))
    ring.drain()
    finish()
    for key in ITEM_ORDER:
        axis, step, _ = ITEMS[key]
        src = quarter_ref(kvb, 0, key[3])
        board.sent(kv_base + ITEM_INDEX[key], src, place.plane(axis, step))
    mark(None)


def rotation_tables():
    frequency = np.power(np.float32(theta), -np.arange(8, dtype=np.float32) / np.float32(8))
    frequency = frequency.astype(np.float32).astype(np.float64)[:, None]
    token = np.arange(1024)[None, :]
    row, col = frequency * (token // GRID_W), frequency * (token % GRID_W)
    table = np.concatenate([np.cos(row), np.sin(row), np.cos(col), np.sin(col)])
    first = frequency * (np.arange(16)[None, :] * 16)
    base = np.stack([np.cos(first), np.sin(first)]).reshape(16, 16).T.reshape(256, 1)
    base = np.broadcast_to(base, (256, 128))
    return base.astype(np.float32), table.astype(np.float32)


def shards(
    latent,
    context,
    cond,
    cond_context,
    mod_weight,
    norm_gain,
    down_q,
    down_kv,
    rope_weight,
    qlat_gain,
    kvlat_gain,
    up_query,
    up_key,
    up_value,
    query_gain,
    key_gain,
    context_bias,
    out_weight,
):
    vmem = pl.BlockSpec(memory_space=pltpu.VMEM)
    smem = pl.BlockSpec(memory_space=pltpu.SMEM)
    copies = len(ITEM_ORDER) + 16 + 8 + 2 + 32 + 2 + 16 + 3 * 16
    base, table = rotation_tables()
    row = lambda v: v.reshape(1, -1)
    fold = lambda v: v.reshape(-1, 128)
    return pl.pallas_call(
        whole_kernel,
        out_shape=jax.ShapeDtypeStruct((64, D), BF),
        in_specs=[vmem] * 16 + [smem] + [vmem] * 3,
        out_specs=vmem,
        scratch_shapes=[
            pltpu.VMEM((8, 128, 768), BF),
            pltpu.VMEM((8, 128, 512), BF),
            pltpu.VMEM((64, D), BF),
            pltpu.VMEM((16, 8, 128), F32),
            pltpu.VMEM((16, 8, 128), F32),
            pltpu.VMEM((16, 160, 128), BF),
            pltpu.VMEM((160, 768), F32),
            pltpu.VMEM((160, 512), F32),
            pltpu.VMEM((64, 768), F32),
            pltpu.VMEM((96, 512), F32),
            pltpu.VMEM((16, 64, 768), BF),
            pltpu.VMEM((16, 64, 640), BF),
            pltpu.VMEM((160, 640), BF),
            pltpu.VMEM((ROPE, 1024), F32),
            pltpu.VMEM((128, 1024), BF),
            pltpu.VMEM((N_UNITS, 2, HEAD + VDIM, 256), BF),
            pltpu.VMEM((16, CTX_DEV, 256), BF),
            pltpu.VMEM((8, 64, D // 2), BF),
            pltpu.VMEM((8, 64, D // 2), BF),
            pltpu.VMEM((512, 1024), F32),
            pltpu.VMEM((512, 1024), F32),
            pltpu.VMEM((1, 1024), F32),
            pltpu.VMEM((1, 1024), F32),
            pltpu.VMEM((1, 1024), F32),
            pltpu.VMEM((1, 1024), F32),
            pltpu.VMEM((VDIM, 1024), F32),
            pltpu.VMEM((8, VDIM, 128), BF),
            pltpu.VMEM((8, VDIM, 128), BF),
            pltpu.VMEM((128, D), F32),
            pltpu.VMEM((64, D), F32),
            pltpu.SemaphoreType.DMA((copies,)),
            pltpu.SemaphoreType.DMA((copies,)),
        ],
        compiler_params=pltpu.CompilerParams(collective_id=0, has_side_effects=True,
                                             vmem_limit_bytes=56 * 1024 * 1024),
        name="whole",
    )(latent, context, fold(cond), fold(cond_context), mod_weight, fold(norm_gain), down_q, down_kv,
      rope_weight.T, fold(qlat_gain), fold(kvlat_gain), up_query.T, up_key.T, up_value.T, row(query_gain),
      row(key_gain), context_bias.reshape(1, 1), out_weight, jnp.asarray(base),
      jnp.asarray(table))


def solution(mesh):
    placed = (
        P(SP_TP, None),
        P("sp", None),
        P(),
        P(),
        P(None, "sp", "tp"),
        P(),
        P("tp", None),
        P("tp", None),
        P(),
        P(),
        P(),
        P(None, "tp"),
        P(None, "tp"),
        P(None, "tp"),
        P(),
        P(),
        P("tp"),
        P("tp", None),
    )
    return jax.shard_map(
        shards, mesh=mesh, in_specs=placed, out_specs=P(SP_TP, None), check_vma=False
    )
```

```python
import math

import jax
import jax.numpy as jnp
import numpy as np
from jax import lax
from jax.experimental import pallas as pl
from jax.experimental.pallas import tpu as pltpu
from jax.sharding import PartitionSpec as P

NOPE = 64
ROPE = 32
HEAD = NOPE + ROPE
VDIM = 64
GRID_W = 64
TOK_DEV = 1024
CTX_DEV = 32
D = 2048
SP_TP = ("sp", "tp")
BF = jnp.bfloat16
F32 = jnp.float32

epsilon = 1e-06
theta = 10000.0
SCALE2 = math.log2(math.e) * HEAD ** (-0.5)
LOG2E = math.log2(math.e)


def exchange_items():
    items = {}
    for h in (0, 1):
        def add(da, db, part, axis, step, trigger):
            names = ("x", "y") if h == 0 else ("y", "x")
            items[(h, da, db, part)] = (names[axis], step, trigger)
        add(-1, 0, "U", 0, 1, None)
        add(1, 0, "U", 0, -1, None)
        add(2, 0, 0, 0, 1, (h, -1, 0, "U"))
        add(2, 0, 1, 0, -1, (h, 1, 0, "U"))
        for da in (0, -1, 1):
            trigger = None if da == 0 else (h, da, 0, "U")
            add(da, -1, "U", 1, 1, trigger)
            add(da, 1, "U", 1, -1, trigger)
            add(da, 2, 0, 1, 1, (h, da, -1, "U"))
            add(da, 2, 1, 1, -1, (h, da, 1, "U"))
        for q in (0, 1):
            add(2, -1, q, 1, 1, (h, 2, 0, q))
            add(2, 1, q, 1, -1, (h, 2, 0, q))
        add(2, 2, 0, 1, 1, (h, 2, -1, 0))
        add(2, 2, 1, 1, -1, (h, 2, 1, 1))
    return items


RELEASE = (10.0, 17.5)
EARLY_AT = 16.0
LOOP_AT = 19.5
STEP = 0.78
UNIT, LATENCY = 3.53, 1.9


def plan_exchange(items):
    free, arrive = {}, {}
    left = dict(items)

    def send(key, at):
        axis, step, _ = items[key]
        begin = max(at, free.get((axis, step), 0.0))
        free[(axis, step)] = begin + (UNIT if key[3] == "U" else UNIT / 2)
        arrive[key] = free[(axis, step)] + LATENCY

    def begin_half(h, at):
        keys = [k for k in items if items[k][2] is None and k[0] == h]
        first = "x" if h == 0 else "y"
        for key in sorted(keys, key=lambda k: 0 if items[k][0] == first else 1):
            send(key, at)

    taken = []

    def rank(key):
        return (round(arrive[key], 1), 0 if key[2] == 0 else 1, str(key))

    def take(now, limit=None):
        got = []
        while True:
            here = sorted((k for k in arrive if k not in taken and arrive[k] <= now), key=rank)
            if not here or (limit is not None and len(got) >= limit):
                return got
            key = here[0]
            taken.append(key)
            got.append(key)
            for other in items:
                if items[other][2] == key:
                    send(other, now)

    begin_half(0, RELEASE[0])
    early = take(EARLY_AT, 3)
    begin_half(1, RELEASE[1])
    now = LOOP_AT
    units = [(0, 0, 0), (1, 0, 0)]
    every = sorted({k[:3] for k in items})

    def ready():
        done = [u for u in every if u not in units
                and all(k in taken for k in items if k[:3] == u)]
        return sorted(done, key=lambda u: (max(arrive[k] for k in items if k[:3] == u), str(u)))

    plan = [take(now)]
    for n in range(1, len(every) + 3, 2):
        got = take(now)
        while len(units) < min(n + 2, len(every) + 2):
            come = ready()
            if come:
                units.append(come[0])
                continue
            now = min(arrive[k] for k in arrive if k not in taken)
            got = got + take(now)
        plan.append(got)
        now += 2 * STEP
    return early, plan, units, now


ITEMS = exchange_items()
EARLY, PLAN, UNITS, PLAN_END = plan_exchange(ITEMS)
ITEM_ORDER = list(ITEMS)
ITEM_INDEX = {k: n for n, k in enumerate(ITEM_ORDER)}
SLOT = {u: n for n, u in enumerate(UNITS)}
N_UNITS = len(UNITS) + 1
CTX_SLOT = len(UNITS)


def mark(name):
    pass


class Board:
    def __init__(self, sends, recvs):
        self.sends, self.recvs, self.count, self.started = sends, recvs, 0, []

    def take(self, n=1):
        first = self.count
        self.count += n
        return first

    def send(self, number, src, dst, device):
        copy = pltpu.make_async_remote_copy(
            src_ref=src, dst_ref=dst, send_sem=self.sends.at[number],
            recv_sem=self.recvs.at[number], device_id=device,
            device_id_type=pl.DeviceIdType.MESH)
        copy.start()

    def arrived(self, number, dst, device):
        pltpu.make_async_remote_copy(
            src_ref=dst, dst_ref=dst, send_sem=self.sends.at[number],
            recv_sem=self.recvs.at[number], device_id=device,
            device_id_type=pl.DeviceIdType.MESH).wait_recv()

    def sent(self, number, src, device):
        pltpu.make_async_remote_copy(
            src_ref=src, dst_ref=src, send_sem=self.sends.at[number],
            recv_sem=self.recvs.at[number], device_id=device,
            device_id_type=pl.DeviceIdType.MESH).wait_send()


CHIPS = (1, -1, 2, -2, 3, -3, 4)


class PlaneShare:
    def __init__(self, board, place, bufs):
        self.board, self.place, self.bufs = board, place, bufs
        self.base = board.take(len(CHIPS) * 4)

    def rows(self, part, offset):
        at = ((self.place.x, self.place.y)[part] + offset + 4) % 4 * 32
        return pl.ds(pl.multiple_of(at, 32), 32)

    def view(self, dist, part, offset):
        return self.bufs[part].at[(self.place.z - dist + 16) % 8, self.rows(part, offset)]

    def number(self, dist, part, kind):
        return self.base + (CHIPS.index(dist) * 2 + part) * 2 + kind

    def device(self, part, step):
        return self.place.plane(("x", "y")[part], step)

    def send(self, dist, part):
        own = self.view(dist, part, 0)
        self.board.send(self.number(dist, part, 0), own, own, self.device(part, 1))
        self.board.send(self.number(dist, part, 1), own, own, self.device(part, -1))

    def arrived(self, dist, part):
        for kind, step in ((0, 1), (1, -1)):
            self.board.arrived(self.number(dist, part, kind), self.view(dist, part, -step),
                               self.device(part, -step))

    def drain(self):
        for dist in CHIPS:
            for part in (0, 1):
                for kind, step in ((0, 1), (1, -1)):
                    self.board.sent(self.number(dist, part, kind), self.view(dist, part, 0),
                                    self.device(part, step))


class Place:
    def __init__(self):
        self.s = lax.axis_index("sp")
        self.t = lax.axis_index("tp")
        self.y, self.x = self.s // 4, self.s % 4
        self.z, self.c = self.t // 2, self.t % 2

    def plane(self, axis, step):
        y, x = self.y, self.x
        if axis == "x":
            x = (x + step + 4) % 4
        else:
            y = (y + step + 4) % 4
        return {"sp": y * 4 + x, "tp": self.t}

    def sp_peer(self, k):
        return {"sp": (self.s + k) % 16, "tp": self.t}

    def tp_peer(self, k):
        return {"sp": self.s, "tp": (self.t + k) % 16}

    def ring(self, step):
        return {"sp": self.s, "tp": ((self.z + step + 8) % 8) * 2 + self.c}

    def sibling(self):
        return {"sp": self.s, "tp": self.z * 2 + 1 - self.c}


def greet(devices):
    barrier = pltpu.get_barrier_semaphore()
    for device in devices:
        pl.semaphore_signal(barrier, inc=1, device_id=device,
                            device_id_type=pl.DeviceIdType.MESH)
    pl.semaphore_wait(barrier, len(devices))


class ZRing:
    def __init__(self, board, place, own, bufs, by_device=False, rows=None):
        self.rows = rows
        self.board, self.place, self.own, self.bufs = board, place, own, bufs
        self.by_device = by_device
        self.base = board.take(16)

    def number(self, way, dist, part):
        return self.base + (0 if way == 1 else 8) + (dist - 1) * 2 + part

    def slot(self, way, dist, part):
        return self.view(part, way * dist)

    def view(self, part, back):
        if self.rows is None:
            return self.bufs[part].at[self.index(back)]
        return self.bufs[part].at[self.index(back), self.rows[part]]

    def index(self, back):
        at = (self.place.z - back + 16) % 8
        return at * 2 + self.place.c if self.by_device else at

    def begin(self):
        for part in (0, 1):
            self.begin_part(part)

    def begin_part(self, part):
        for way in (1, -1):
            self.board.send(self.number(way, 1, part), self.own[part],
                            self.view(part, 0), self.place.ring(way))

    def take(self, way, dist, part):
        here = self.slot(way, dist, part)
        self.board.arrived(self.number(way, dist, part), here, self.place.ring(-way))
        if dist < 3 or (dist == 3 and part == (0 if way == 1 else 1)):
            self.board.send(self.number(way, dist + 1, part), here, here, self.place.ring(way))

    def items(self):
        out = []
        for dist in (1, 2, 3):
            for part in (0, 1):
                for way in (1, -1):
                    out.append((way, dist, part))
        out.append((1, 4, 0))
        out.append((-1, 4, 1))
        return out

    def drain(self):
        for part in (0, 1):
            for way in (1, -1):
                self.board.sent(self.number(way, 1, part), self.own[part], self.place.ring(way))
        for way, dist, part in self.items():
            if dist > 1:
                here = self.slot(way, dist - 1, part)
                self.board.sent(self.number(way, dist, part), here, self.place.ring(way))


def quarter_ref(buf, slot, part):
    if part == "U":
        return buf.at[slot]
    return buf.at[slot, part]


def whole_kernel(lat_ref, context_ref, cond_ref, condc_ref, mw_ref, ng_ref, dq_ref, dkv_ref,
                 rw_ref, qlg_ref, kvlg_ref, upq_ref, upk_ref, upv_ref, qg_ref, kg_ref, bias_ref,
                 ow_ref, base_ref, tab_ref, out_ref,
                 wq, wkv, latsib, modp, modf, xn, uq, ukv, sq, skv, lq, lk, wk, rt,
                 qt, kvb, cbuf, owa, owb, s_a, s_b, mb_a, mb_b, m_ref, l_ref, acc, att, attb,
                 part_ref, sib_ref, sends, recvs):
    place = Place()
    board = Board(sends, recvs)
    kv_base = board.take(len(ITEM_ORDER))
    ctx_base = board.take(16)
    a2a_base = board.take(8)
    d2d = board.take(1)
    lat_d2d = board.take(1)
    modp_base = board.take(16)
    modf_base = board.take(16)
    part_base = board.take(2)
    share_base = board.take(16)
    half_cols = D // 2
    ring = ZRing(board, place, (ow_ref.at[:, :half_cols], ow_ref.at[:, half_cols:]), (owa, owb))
    share_w = PlaneShare(board, place, (wq, wkv))
    quarter = (share_w.rows(0, 0), share_w.rows(1, 0))
    wring = ZRing(board, place, (dq_ref.at[quarter[0]], dkv_ref.at[quarter[1]]), (wq, wkv),
                  rows=quarter)
    facing = (share_w.rows(0, 2), share_w.rows(1, 2))
    oring = ZRing(board, place, (dq_ref.at[facing[0]], dkv_ref.at[facing[1]]), (wq, wkv),
                  rows=facing)
    lring = ZRing(board, place, (lk.at[place.t], lq.at[place.t]), (lk, lq), by_device=True)

    mark("a_greet")
    greet([place.sp_peer(k) for k in range(1, 16)] + [place.tp_peer(k) for k in range(1, 16)])

    mark("b_mod")
    wring.begin()
    oring.begin()
    board.send(lat_d2d, lat_ref, latsib, place.sibling())

    def silu(ref):
        rows = lax.broadcasted_iota(jnp.int32, (16, 128), 0)
        v = jnp.sum(jnp.where(rows == place.s, ref[...].astype(F32), 0.0), axis=0, keepdims=True)
        return v / (1.0 + jnp.exp(-v))

    act = jnp.concatenate(
        [silu(cond_ref), silu(condc_ref), jnp.zeros((14, 128), F32)],
        axis=0).astype(BF)
    terms = [jnp.dot(act, mw_ref[r], preferred_element_type=F32) for r in range(3)]
    modp[place.s] = jnp.concatenate(
        [terms[0][0:1], terms[1][0:1], terms[2][0:1], terms[0][1:2], terms[1][1:2],
         jnp.zeros((3, 128), F32)], axis=0)
    for k in range(1, 16):
        board.send(modp_base + k, modp.at[place.s], modp.at[place.s], place.sp_peer(k))

    mark("c_local")
    wq[place.z] = dq_ref[...]
    wkv[place.z] = dkv_ref[...]
    owa[place.z] = ow_ref[:, :half_cols]
    owb[place.z] = ow_ref[:, half_cols:]
    wk[...] = jnp.zeros(wk.shape, BF)
    wk[0:NOPE, 0:512] = upk_ref[...]
    wk[HEAD:HEAD + VDIM, 0:512] = upv_ref[...]
    unit = (lax.broadcasted_iota(jnp.int32, (ROPE, 128), 0)
            == lax.broadcasted_iota(jnp.int32, (ROPE, 128), 1))
    wk[NOPE:HEAD, 512:640] = jnp.where(unit, 1.0, 0.0).astype(BF)

    def inverse(ref):
        rows = ref[...].astype(F32)
        return lax.rsqrt(jnp.mean(rows * rows, axis=-1, keepdims=True) + epsilon)

    inv_own = inverse(lat_ref)
    inv_ctx = inverse(context_ref)

    mark("d_modwait")
    def from_ring(dist):
        for part in (0, 1):
            if dist == 4:
                wring.take(1 if part == 0 else -1, 4, part)
                share_w.send(4, part)
                continue
            for way in (1, -1):
                wring.take(way, dist, part)
                share_w.send(way * dist, part)

    def facing_ring(dist):
        for part in (0, 1):
            for way in ((1 if part == 0 else -1,) if dist == 4 else (1, -1)):
                oring.take(way, dist, part)

    from_ring(1)
    facing_ring(1)
    for k in range(1, 16):
        board.arrived(modp_base + k, modp.at[(place.s - k + 16) % 16], place.sp_peer(16 - k))
    modf[place.t] = jnp.sum(modp[...], axis=0)
    for k in range(1, 16):
        board.send(modf_base + k, modf.at[place.t], modf.at[place.t], place.tp_peer(k))

    board.arrived(lat_d2d, latsib, place.sibling())
    inv_sib = inverse(latsib)
    from_ring(2)
    facing_ring(2)
    mark("e_modfwait")
    for k in range(1, 16):
        board.arrived(modf_base + k, modf.at[(place.t - k + 16) % 16], place.tp_peer(16 - k))

    mark("f_norm")
    norm_gain = ng_ref[...].astype(F32)
    for k in range(16):
        cols = slice(k * 128, (k + 1) * 128)
        gain = norm_gain[k:k + 1]
        shift, scale = modf[k, 0:1, :], modf[k, 1:2, :]
        own = lat_ref[:, cols].astype(F32) * inv_own * gain
        xn[k, 0:64] = (own * (1.0 + scale) + shift).astype(BF)
        sib = latsib[:, cols].astype(F32) * inv_sib * gain
        xn[k, 96:160] = (sib * (1.0 + scale) + shift).astype(BF)
        ctx = context_ref[:, cols].astype(F32) * inv_ctx * gain
        xn[k, 64:96] = (ctx * (1.0 + modf[k, 4:5, :]) + modf[k, 3:4, :]).astype(BF)

    def add_product(at, part):
        rows = xn[2 * at + place.c]
        if part == 0:
            uq[...] += jnp.dot(rows, wq[at], preferred_element_type=F32)
        else:
            ukv[...] += jnp.dot(rows, wkv[at], preferred_element_type=F32)

    uq[...] = jnp.dot(xn[place.t], wq[place.z], preferred_element_type=F32)
    ukv[...] = jnp.dot(xn[place.t], wkv[place.z], preferred_element_type=F32)
    contract = (((1,), (1,)), ((), ()))
    rope = jnp.zeros((96, ROPE), F32)
    for k in range(16):
        rope = rope + lax.dot_general(xn[k, 0:96], rw_ref[:, k * 128:(k + 1) * 128], contract,
                                      preferred_element_type=F32)
    rope = rope.astype(BF).astype(F32)
    mark("g_wring")
    def finish_chip(dist):
        for part in (0, 1):
            for d in ((4,) if dist == 4 else (dist, -dist)):
                share_w.arrived(d, part)
                add_product((place.z - d + 16) % 8, part)

    from_ring(3)
    finish_chip(1)
    facing_ring(3)
    finish_chip(2)
    from_ring(4)
    finish_chip(3)
    facing_ring(4)
    finish_chip(4)

    mark("h_d2dpart")
    board.send(part_base + 1, ukv.at[64:160], skv, place.sibling())
    board.send(part_base, uq.at[96:160], sq, place.sibling())

    def latent_of(total, gain_ref):
        gain = gain_ref[...].astype(F32)
        gain = jnp.concatenate([gain[k:k + 1] for k in range(gain.shape[0])], axis=1)
        return (total * lax.rsqrt(jnp.mean(total * total, axis=-1, keepdims=True) + epsilon)
                * gain).astype(BF)

    board.arrived(part_base + 1, skv, place.sibling())
    lk[place.t, :, 0:512] = latent_of(ukv[0:64] + skv[32:96], kvlg_ref)
    lk[place.t, :, 512:640] = jnp.concatenate(
        [rope[0:64], jnp.zeros((64, 96), F32)], axis=1).astype(BF)
    def share(number, ref):
        board.send(share_base + number, ref, ref, place.sibling())

    lring.begin_part(0)
    share(0, lk.at[place.t])
    board.arrived(part_base, sq, place.sibling())
    lq[place.t] = latent_of(uq[0:64] + sq[...], qlg_ref)
    lring.begin_part(1)
    share(1, lq.at[place.t])

    mark("i_ctx")
    ctx_kv = latent_of(ukv[64:96] + skv[0:32], kvlg_ref)
    ctx_k = lax.dot_general(ctx_kv, upk_ref[...], contract, preferred_element_type=F32)
    ctx_v = lax.dot_general(ctx_kv, upv_ref[...], contract, preferred_element_type=F32)
    ctx_u = jnp.concatenate([ctx_k, rope[64:96]], axis=1)
    ctx_n = ctx_u * lax.rsqrt(jnp.mean(ctx_u * ctx_u, axis=-1, keepdims=True) + epsilon)
    ctx_n = ctx_n * kg_ref[...]
    cbuf[place.s] = jnp.concatenate(
        [ctx_n, jnp.zeros((CTX_DEV, 128 - HEAD), F32), ctx_v,
         jnp.zeros((CTX_DEV, 128 - VDIM), F32)], axis=1).astype(BF)
    for k in range(1, 16):
        board.send(ctx_base + k, cbuf.at[place.s], cbuf.at[place.s], place.sp_peer(k))

    base = base_ref[pl.ds(pl.multiple_of(place.s * 16, 16), 16)]
    base_cos, base_sin = base[0:8, 0:1], base[8:16, 0:1]
    rt[0:8] = tab_ref[0:8] * base_cos - tab_ref[8:16] * base_sin
    rt[8:16] = tab_ref[8:16] * base_cos + tab_ref[0:8] * base_sin
    rt[16:32] = tab_ref[16:32]

    def column(gain_ref):
        row = jnp.concatenate([gain_ref[...], jnp.zeros((1, 128 - HEAD), F32)], axis=1)
        return jnp.broadcast_to(row, (128, 128)).T[0:HEAD, 0:1]

    def turned(u, gain, cols):
        row_cos, row_sin = rt[0:8, cols], rt[8:16, cols]
        col_cos, col_sin = rt[16:24, cols], rt[24:32, cols]
        normal = u * lax.rsqrt(jnp.mean(u * u, axis=0, keepdims=True) + epsilon) * gain
        a, b, c, d = (normal[NOPE + 8 * n:NOPE + 8 * n + 8] for n in range(4))
        return jnp.concatenate(
            [normal[0:NOPE], a * row_cos - b * row_sin, b * row_cos + a * row_sin,
             c * col_cos - d * col_sin, d * col_cos + c * col_sin], axis=0)

    query_gain, key_gain = column(qg_ref), column(kg_ref)

    def finish():
        wring.drain()
        oring.drain()
        share_w.drain()
        lring.drain()
        board.sent(lat_d2d, lat_ref, place.sibling())
        for k in range(1, 16):
            board.sent(modp_base + k, modp.at[place.s], place.sp_peer(k))
            board.sent(modf_base + k, modf.at[place.t], place.tp_peer(k))
        board.sent(part_base, uq.at[96:160], place.sibling())
        board.sent(part_base + 1, ukv.at[64:160], place.sibling())
        share_sizes = [0, 1] + [item[2] for item in l_items]
        for n, part in enumerate(share_sizes):
            board.sent(share_base + n, (lk, lq)[part].at[0], place.sibling())

    def kv_send(key, src):
        axis, step, _ = ITEMS[key]
        h, da, db, part = key
        board.send(kv_base + ITEM_INDEX[key], src, quarter_ref(kvb, SLOT[key[:3]], part),
                   place.plane(axis, step))

    def own_part(h):
        return kvb.at[SLOT[(h, 0, 0)]]

    def kv_begin(h):
        for key in sorted((k for k in ITEMS if ITEMS[k][2] is None and k[0] == h),
                          key=lambda k: 0 if ITEMS[k][0] == ("x" if k[0] == 0 else "y") else 1):
            kv_send(key, own_part(h))

    def kv_take(key):
        axis, step, _ = ITEMS[key]
        here = quarter_ref(kvb, SLOT[key[:3]], key[3])
        board.arrived(kv_base + ITEM_INDEX[key], here, place.plane(axis, -step))
        for other in ITEM_ORDER:
            if ITEMS[other][2] == key:
                src = here
                if key[3] == "U" and other[3] != "U":
                    src = kvb.at[SLOT[key[:3]], other[3]]
                kv_send(other, src)

    mark("j_lring")
    l_items = lring.items()
    other = 1 - place.c

    def ring_take(way, dist, part):
        lring.take(way, dist, part)
        share(2 + l_items.index((way, dist, part)), lring.slot(way, dist, part))

    def chip(dist, part):
        at = (place.z - dist + 16) % 8
        if dist == 0:
            number = part
        elif dist == 4:
            number = 2 + l_items.index((1 if part == 0 else -1, 4, part))
        else:
            number = 2 + l_items.index((1 if dist > 0 else -1, abs(dist), part))
        buf = (lk, lq)[part]
        board.arrived(share_base + number, buf.at[at * 2 + other], place.sibling())
        cols = pl.ds(pl.multiple_of(at * 128, 128), 128)
        return buf[pl.ds(at * 2, 2)].reshape(128, buf.shape[2]), cols

    def chip_keys(dist, h, n):
        rows, cols = chip(dist, 0)
        kv = lax.dot_general(wk[...], rows, contract, preferred_element_type=F32)
        kv = jnp.concatenate([turned(kv[0:HEAD], key_gain, cols), kv[HEAD:HEAD + VDIM]], axis=0)
        kvb[SLOT[(h, 0, 0)], n // 2, :, (n % 2) * 128:(n % 2) * 128 + 128] = kv.astype(BF)

    def chip_queries(dist):
        rows, cols = chip(dist, 1)
        u = lax.dot_general(upq_ref[...], rows, contract, preferred_element_type=F32)
        qt[0:HEAD, cols] = turned(u, query_gain, cols).astype(BF)

    qt[HEAD:128] = jnp.zeros((128 - HEAD, 1024), BF)
    ring_take(1, 1, 0)
    ring_take(-1, 1, 0)
    chip_keys(0, 0, 0)
    ring_take(1, 1, 1)
    ring_take(-1, 1, 1)
    chip_keys(1, 0, 1)
    chip_keys(-1, 0, 2)
    ring_take(1, 2, 0)
    ring_take(-1, 2, 0)
    chip_queries(0)
    chip_keys(2, 0, 3)
    mark("k_h0")
    kv_begin(0)
    ring_take(1, 2, 1)
    ring_take(-1, 2, 1)
    chip_queries(1)
    chip_queries(-1)
    ring_take(1, 3, 0)
    ring_take(-1, 3, 0)
    chip_keys(-2, 1, 0)
    chip_queries(2)
    ring_take(1, 3, 1)
    ring_take(-1, 3, 1)
    ring.begin()
    chip_keys(3, 1, 1)
    chip_keys(-3, 1, 2)
    chip_queries(-2)
    mark("l_early")
    for key in EARLY:
        kv_take(key)
    mark("l_h1")
    ring_take(1, 4, 0)
    chip_keys(4, 1, 3)
    kv_begin(1)
    mark("l_q")
    chip_queries(3)
    chip_queries(-3)
    ring_take(-1, 4, 1)
    chip_queries(4)

    def ctx_unit():
        for k in range(1, 16):
            board.arrived(ctx_base + k, cbuf.at[(place.s - k + 16) % 16], place.sp_peer(16 - k))
        turned = cbuf[...].reshape(512, 256).astype(F32).T.astype(BF)
        for q in (0, 1):
            kvb[CTX_SLOT, q, 0:HEAD, :] = turned[0:HEAD, q * 256:(q + 1) * 256]
            kvb[CTX_SLOT, q, HEAD:HEAD + VDIM, :] = turned[128:128 + VDIM, q * 256:(q + 1) * 256]

    mark("m_init")
    m_ref[...] = jnp.full(m_ref.shape, -jnp.inf, F32)
    l_ref[...] = jnp.zeros(l_ref.shape, F32)
    acc[...] = jnp.zeros(acc.shape, F32)

    def products(slot, s_ref, mb_ref):
        for q in (0, 1):
            keys = kvb[slot, q, 0:128, :].T
            for n in range(4):
                cols = slice(n * 256, (n + 1) * 256)
                scores = jnp.dot(keys, qt[:, cols], preferred_element_type=F32)
                s_ref[q * 256:(q + 1) * 256, cols] = scores
                top = jnp.max(scores, axis=0, keepdims=True)
                mb_ref[:, cols] = top if q == 0 else jnp.maximum(mb_ref[:, cols], top)

    def absorb(slot, s_ref, mb_ref, bias):
        for n in range(4):
            cols = slice(n * 256, (n + 1) * 256)
            old = m_ref[:, cols]
            top = mb_ref[:, cols] * SCALE2
            if bias is not None:
                top = top + bias
            new = jnp.maximum(old, top)
            m_ref[:, cols] = new
            factor = jnp.exp2(old - new)
            less = new if bias is None else new - bias
            weights = jnp.exp2(s_ref[:, cols] * SCALE2 - less)
            l_ref[:, cols] = l_ref[:, cols] * factor + jnp.sum(weights, axis=0, keepdims=True)
            rounded = weights.astype(BF)
            summed = jnp.dot(kvb[slot, 0, HEAD:HEAD + VDIM, :], rounded[:256],
                             preferred_element_type=F32)
            summed = summed + jnp.dot(kvb[slot, 1, HEAD:HEAD + VDIM, :], rounded[256:],
                                      preferred_element_type=F32)
            acc[:, cols] = acc[:, cols] * factor + summed

    ring_items = ring.items()
    ring_plan = [[] for _ in range(17)]
    for n, item in enumerate(ring_items):
        ring_plan[min(2 + (n * 13) // len(ring_items), 16)].append(item)

    def actions(n):
        for key in PLAN[n]:
            kv_take(key)
        for item in ring_plan[n]:
            ring.take(*item)

    mark("n_prolog")
    actions(0)
    products(0, s_a, mb_a)
    for i in range(16):
        mark(f"o{i:02d}a")
        actions(i + 1)
        if i == 15:
            ctx_unit()
        mark(f"o{i:02d}b")
        products(2 * i + 1, s_b, mb_b)
        absorb(2 * i, s_a, mb_a, None)
        products(2 * i + 2, s_a, mb_a)
        absorb(2 * i + 1, s_b, mb_b, None)
    mark("p_last")
    bias = (bias_ref[0, 0] + math.log(TOK_DEV / CTX_DEV)) * LOG2E
    absorb(CTX_SLOT, s_a, mb_a, bias)

    mark("q_a2a")
    for k in range(8):
        cols = slice(k * 128, (k + 1) * 128)
        att[k] = (acc[:, cols] / l_ref[:, cols]).astype(BF)
    for k in range(1, 8):
        board.send(a2a_base + k, att.at[(place.z + k) % 8], attb.at[place.z], place.ring(k))
    attb[place.z] = att[place.z]
    for k in range(1, 8):
        board.arrived(a2a_base + k, attb.at[(place.z - k + 8) % 8], place.ring(-k))
    mark("r_out")
    rows = attb[...].reshape(8 * VDIM, 128).astype(F32).T.astype(BF)
    for n, weight in enumerate((owa, owb)):
        part_ref[:, n * half_cols:(n + 1) * half_cols] = jnp.dot(
            rows, weight[...].reshape(8 * VDIM, half_cols), preferred_element_type=F32)
    away = part_ref.at[pl.ds(pl.multiple_of(64 * (1 - place.c), 64), 64)]
    mark("s_d2d")
    board.send(d2d, away, sib_ref, place.sibling())
    board.arrived(d2d, sib_ref, place.sibling())
    gates = jnp.concatenate([modf[k, 2:3, :] for k in range(16)], axis=1)
    mine = part_ref[pl.ds(pl.multiple_of(64 * place.c, 64), 64)]
    projected = mine + sib_ref[...]
    out_ref[...] = (lat_ref[...].astype(F32) + gates * projected).astype(BF)

    mark("t_drain")
    board.sent(d2d, away, place.sibling())
    for k in range(1, 8):
        board.sent(a2a_base + k, att.at[(place.z + k) % 8], place.ring(k))
    for k in range(1, 16):
        board.sent(ctx_base + k, cbuf.at[place.s], place.sp_peer(k))
    ring.drain()
    finish()
    for key in ITEM_ORDER:
        axis, step, _ = ITEMS[key]
        src = quarter_ref(kvb, 0, key[3])
        board.sent(kv_base + ITEM_INDEX[key], src, place.plane(axis, step))
    mark(None)


def rotation_tables():
    frequency = np.power(np.float32(theta), -np.arange(8, dtype=np.float32) / np.float32(8))
    frequency = frequency.astype(np.float32).astype(np.float64)[:, None]
    token = np.arange(1024)[None, :]
    row, col = frequency * (token // GRID_W), frequency * (token % GRID_W)
    table = np.concatenate([np.cos(row), np.sin(row), np.cos(col), np.sin(col)])
    first = frequency * (np.arange(16)[None, :] * 16)
    base = np.stack([np.cos(first), np.sin(first)]).reshape(16, 16).T.reshape(256, 1)
    base = np.broadcast_to(base, (256, 128))
    return base.astype(np.float32), table.astype(np.float32)


def shards(
    latent,
    context,
    cond,
    cond_context,
    mod_weight,
    norm_gain,
    down_q,
    down_kv,
    rope_weight,
    qlat_gain,
    kvlat_gain,
    up_query,
    up_key,
    up_value,
    query_gain,
    key_gain,
    context_bias,
    out_weight,
):
    vmem = pl.BlockSpec(memory_space=pltpu.VMEM)
    smem = pl.BlockSpec(memory_space=pltpu.SMEM)
    copies = len(ITEM_ORDER) + 16 + 8 + 2 + 32 + 2 + 16 + 4 * 16 + 28
    base, table = rotation_tables()
    row = lambda v: v.reshape(1, -1)
    fold = lambda v: v.reshape(-1, 128)
    return pl.pallas_call(
        whole_kernel,
        out_shape=jax.ShapeDtypeStruct((64, D), BF),
        in_specs=[vmem] * 16 + [smem] + [vmem] * 3,
        out_specs=vmem,
        scratch_shapes=[
            pltpu.VMEM((8, 128, 768), BF),
            pltpu.VMEM((8, 128, 512), BF),
            pltpu.VMEM((64, D), BF),
            pltpu.VMEM((16, 8, 128), F32),
            pltpu.VMEM((16, 8, 128), F32),
            pltpu.VMEM((16, 160, 128), BF),
            pltpu.VMEM((160, 768), F32),
            pltpu.VMEM((160, 512), F32),
            pltpu.VMEM((64, 768), F32),
            pltpu.VMEM((96, 512), F32),
            pltpu.VMEM((16, 64, 768), BF),
            pltpu.VMEM((16, 64, 640), BF),
            pltpu.VMEM((160, 640), BF),
            pltpu.VMEM((ROPE, 1024), F32),
            pltpu.VMEM((128, 1024), BF),
            pltpu.VMEM((N_UNITS, 2, HEAD + VDIM, 256), BF),
            pltpu.VMEM((16, CTX_DEV, 256), BF),
            pltpu.VMEM((8, 64, D // 2), BF),
            pltpu.VMEM((8, 64, D // 2), BF),
            pltpu.VMEM((512, 1024), F32),
            pltpu.VMEM((512, 1024), F32),
            pltpu.VMEM((1, 1024), F32),
            pltpu.VMEM((1, 1024), F32),
            pltpu.VMEM((1, 1024), F32),
            pltpu.VMEM((1, 1024), F32),
            pltpu.VMEM((VDIM, 1024), F32),
            pltpu.VMEM((8, VDIM, 128), BF),
            pltpu.VMEM((8, VDIM, 128), BF),
            pltpu.VMEM((128, D), F32),
            pltpu.VMEM((64, D), F32),
            pltpu.SemaphoreType.DMA((copies,)),
            pltpu.SemaphoreType.DMA((copies,)),
        ],
        compiler_params=pltpu.CompilerParams(collective_id=0, has_side_effects=True,
                                             vmem_limit_bytes=56 * 1024 * 1024),
        name="whole",
    )(latent, context, fold(cond), fold(cond_context), mod_weight, fold(norm_gain), down_q, down_kv,
      rope_weight.T, fold(qlat_gain), fold(kvlat_gain), up_query.T, up_key.T, up_value.T, row(query_gain),
      row(key_gain), context_bias.reshape(1, 1), out_weight, jnp.asarray(base),
      jnp.asarray(table))


def solution(mesh):
    placed = (
        P(SP_TP, None),
        P("sp", None),
        P(),
        P(),
        P(None, "sp", "tp"),
        P(),
        P("tp", None),
        P("tp", None),
        P(),
        P(),
        P(),
        P(None, "tp"),
        P(None, "tp"),
        P(None, "tp"),
        P(),
        P(),
        P("tp"),
        P("tp", None),
    )
    return jax.shard_map(
        shards, mesh=mesh, in_specs=placed, out_specs=P(SP_TP, None), check_vma=False
    )
```

```python
import math

import jax
import jax.numpy as jnp
import numpy as np
from jax import lax
from jax.experimental import pallas as pl
from jax.experimental.pallas import tpu as pltpu
from jax.sharding import PartitionSpec as P

NOPE = 64
ROPE = 32
HEAD = NOPE + ROPE
VDIM = 64
GRID_W = 64
TOK_DEV = 1024
CTX_DEV = 32
D = 2048
SP_TP = ("sp", "tp")
BF = jnp.bfloat16
F32 = jnp.float32

epsilon = 1e-06
theta = 10000.0
SCALE2 = math.log2(math.e) * HEAD ** (-0.5)
LOG2E = math.log2(math.e)


def exchange_items():
    items = {}
    for h in (0, 1):
        for q in (0, 1):
            def add(da, db, part, axis, step, trigger):
                names = ("x", "y") if q == 0 else ("y", "x")
                trigger = None if trigger is None else (h, q) + trigger
                items[(h, q, da, db, part)] = (names[axis], step, trigger)
            add(-1, 0, "U", 0, 1, None)
            add(1, 0, "U", 0, -1, None)
            add(2, 0, 0, 0, 1, (-1, 0, "U"))
            add(2, 0, 1, 0, -1, (1, 0, "U"))
            for da in (0, -1, 1):
                trigger = None if da == 0 else (da, 0, "U")
                add(da, -1, "U", 1, 1, trigger)
                add(da, 1, "U", 1, -1, trigger)
                add(da, 2, 0, 1, 1, (da, -1, "U"))
                add(da, 2, 1, 1, -1, (da, 1, "U"))
            for part in (0, 1):
                add(2, -1, part, 1, 1, (2, 0, part))
                add(2, 1, part, 1, -1, (2, 0, part))
            add(2, 2, 0, 1, 1, (2, -1, 0))
            add(2, 2, 1, 1, -1, (2, 1, 1))
    return items


def unit_of(key):
    h, q, da, db, _ = key
    return (h, da, db) if q == 0 else (h, db, da)


RELEASE = (9.0, 17.4)
LOOKS = (13.2, 16.0, 18.8)
LOOP_AT = 20.2
STEP = 0.79
UNIT, LATENCY = 1.85, 2.0


def plan_exchange(items):
    free, arrive = {}, {}
    taken = []

    def send(key, at):
        axis, step, _ = items[key]
        begin = max(at, free.get((axis, step), 0.0))
        free[(axis, step)] = begin + (UNIT if key[4] == "U" else UNIT / 2)
        arrive[key] = free[(axis, step)] + LATENCY

    def begin_half(h, at):
        for key in own_keys(items, h):
            send(key, at)

    def rank(key):
        return (round(arrive[key], 1), 0 if key[3] == 0 else 1, str(key))

    def take(now):
        got = []
        while True:
            here = sorted((k for k in arrive if k not in taken and arrive[k] <= now), key=rank)
            if not here:
                return got
            key = here[0]
            taken.append(key)
            got.append(key)
            for other in items:
                if items[other][2] == key:
                    send(other, now)

    begin_half(0, RELEASE[0])
    early = [take(LOOKS[0]), take(LOOKS[1])]
    begin_half(1, RELEASE[1])
    early.append(take(LOOKS[2]))
    now = LOOP_AT
    units = [(0, 0, 0), (1, 0, 0)]
    every = sorted({unit_of(k) for k in items})

    def come(u):
        return max(arrive[k] for k in items if unit_of(k) == u)

    def ready():
        done = [u for u in every if u not in units
                and all(k in taken for k in items if unit_of(k) == u)]
        return sorted(done, key=lambda u: (come(u), str(u)))

    plan = [take(now)]
    for n in range(1, len(every) + 3, 2):
        got = take(now)
        while len(units) < min(n + 2, len(every) + 2):
            found = ready()
            if found:
                units.append(found[0])
                continue
            now = min(arrive[k] for k in arrive if k not in taken)
            got = got + take(now)
        plan.append(got)
        now += 2 * STEP
    return early, plan, units, now


def own_keys(items, h):
    keys = [k for k in items if items[k][2] is None and k[0] == h]
    return sorted(keys, key=lambda k: 0 if items[k][0] == ("x", "y")[k[1]] else 1)


ITEMS = exchange_items()
EARLY, PLAN, UNITS, PLAN_END = plan_exchange(ITEMS)
ITEM_ORDER = list(ITEMS)
ITEM_INDEX = {k: n for n, k in enumerate(ITEM_ORDER)}
SLOT = {u: n for n, u in enumerate(UNITS)}
N_UNITS = len(UNITS) + 1
CTX_SLOT = len(UNITS)


def mark(name):
    pass


class Board:
    def __init__(self, sends, recvs):
        self.sends, self.recvs, self.count, self.started = sends, recvs, 0, []

    def take(self, n=1):
        first = self.count
        self.count += n
        return first

    def send(self, number, src, dst, device):
        copy = pltpu.make_async_remote_copy(
            src_ref=src, dst_ref=dst, send_sem=self.sends.at[number],
            recv_sem=self.recvs.at[number], device_id=device,
            device_id_type=pl.DeviceIdType.MESH)
        copy.start()

    def arrived(self, number, dst, device):
        pltpu.make_async_remote_copy(
            src_ref=dst, dst_ref=dst, send_sem=self.sends.at[number],
            recv_sem=self.recvs.at[number], device_id=device,
            device_id_type=pl.DeviceIdType.MESH).wait_recv()

    def sent(self, number, src, device):
        pltpu.make_async_remote_copy(
            src_ref=src, dst_ref=src, send_sem=self.sends.at[number],
            recv_sem=self.recvs.at[number], device_id=device,
            device_id_type=pl.DeviceIdType.MESH).wait_send()


CHIPS = (1, -1, 2, -2, 3, -3, 4)


class PlaneShare:
    def __init__(self, board, place, bufs):
        self.board, self.place, self.bufs = board, place, bufs
        self.base = board.take(len(CHIPS) * 4)

    def rows(self, part, offset):
        at = ((self.place.x, self.place.y)[part] + offset + 4) % 4 * 32
        return pl.ds(pl.multiple_of(at, 32), 32)

    def view(self, dist, part, offset):
        return self.bufs[part].at[(self.place.z - dist + 16) % 8, self.rows(part, offset)]

    def number(self, dist, part, kind):
        return self.base + (CHIPS.index(dist) * 2 + part) * 2 + kind

    def device(self, part, step):
        return self.place.plane(("x", "y")[part], step)

    def send(self, dist, part):
        own = self.view(dist, part, 0)
        self.board.send(self.number(dist, part, 0), own, own, self.device(part, 1))
        self.board.send(self.number(dist, part, 1), own, own, self.device(part, -1))

    def arrived(self, dist, part):
        for kind, step in ((0, 1), (1, -1)):
            self.board.arrived(self.number(dist, part, kind), self.view(dist, part, -step),
                               self.device(part, -step))

    def drain(self):
        for dist in CHIPS:
            for part in (0, 1):
                for kind, step in ((0, 1), (1, -1)):
                    self.board.sent(self.number(dist, part, kind), self.view(dist, part, 0),
                                    self.device(part, step))


class Place:
    def __init__(self):
        self.s = lax.axis_index("sp")
        self.t = lax.axis_index("tp")
        self.y, self.x = self.s // 4, self.s % 4
        self.z, self.c = self.t // 2, self.t % 2

    def plane(self, axis, step):
        y, x = self.y, self.x
        if axis == "x":
            x = (x + step + 4) % 4
        else:
            y = (y + step + 4) % 4
        return {"sp": y * 4 + x, "tp": self.t}

    def sp_peer(self, k):
        return {"sp": (self.s + k) % 16, "tp": self.t}

    def tp_peer(self, k):
        return {"sp": self.s, "tp": (self.t + k) % 16}

    def ring(self, step):
        return {"sp": self.s, "tp": ((self.z + step + 8) % 8) * 2 + self.c}

    def sibling(self):
        return {"sp": self.s, "tp": self.z * 2 + 1 - self.c}


def greet(devices):
    barrier = pltpu.get_barrier_semaphore()
    for device in devices:
        pl.semaphore_signal(barrier, inc=1, device_id=device,
                            device_id_type=pl.DeviceIdType.MESH)
    pl.semaphore_wait(barrier, len(devices))


class ZRing:
    def __init__(self, board, place, own, bufs, by_device=False, rows=None):
        self.rows = rows
        self.board, self.place, self.own, self.bufs = board, place, own, bufs
        self.by_device = by_device
        self.base = board.take(16)

    def number(self, way, dist, part):
        return self.base + (0 if way == 1 else 8) + (dist - 1) * 2 + part

    def slot(self, way, dist, part):
        return self.view(part, way * dist)

    def view(self, part, back):
        if self.rows is None:
            return self.bufs[part].at[self.index(back)]
        return self.bufs[part].at[self.index(back), self.rows[part]]

    def index(self, back):
        at = (self.place.z - back + 16) % 8
        return at * 2 + self.place.c if self.by_device else at

    def begin(self):
        for part in (0, 1):
            self.begin_part(part)

    def begin_part(self, part):
        for way in (1, -1):
            self.board.send(self.number(way, 1, part), self.own[part],
                            self.view(part, 0), self.place.ring(way))

    def take(self, way, dist, part):
        here = self.slot(way, dist, part)
        self.board.arrived(self.number(way, dist, part), here, self.place.ring(-way))
        if dist < 3 or (dist == 3 and part == (0 if way == 1 else 1)):
            self.board.send(self.number(way, dist + 1, part), here, here, self.place.ring(way))

    def items(self):
        out = []
        for dist in (1, 2, 3):
            for part in (0, 1):
                for way in (1, -1):
                    out.append((way, dist, part))
        out.append((1, 4, 0))
        out.append((-1, 4, 1))
        return out

    def drain(self):
        for part in (0, 1):
            for way in (1, -1):
                self.board.sent(self.number(way, 1, part), self.own[part], self.place.ring(way))
        for way, dist, part in self.items():
            if dist > 1:
                here = self.slot(way, dist - 1, part)
                self.board.sent(self.number(way, dist, part), here, self.place.ring(way))


def quarter_ref(buf, slot, quarter, part):
    if part == "U":
        return buf.at[slot, quarter]
    return buf.at[slot, quarter, :, 128 * part:128 * part + 128]


def whole_kernel(lat_ref, context_ref, cond_ref, condc_ref, mw_ref, ng_ref, dq_ref, dkv_ref,
                 rw_ref, qlg_ref, kvlg_ref, upq_ref, upk_ref, upv_ref, qg_ref, kg_ref, bias_ref,
                 ow_ref, base_ref, tab_ref, out_ref,
                 wq, wkv, latsib, modp, modf, xn, uq, ukv, sq, skv, lq, lk, wk, rt,
                 qt, kvb, cbuf, owa, owb, s_a, s_b, mb_a, mb_b, m_ref, l_ref, acc, att, attb,
                 part_ref, sib_ref, sends, recvs):
    place = Place()
    board = Board(sends, recvs)
    kv_base = board.take(len(ITEM_ORDER))
    ctx_base = board.take(16)
    a2a_base = board.take(8)
    d2d = board.take(1)
    lat_d2d = board.take(1)
    modp_base = board.take(16)
    modf_base = board.take(16)
    part_base = board.take(2)
    share_base = board.take(16)
    half_cols = D // 2
    ring = ZRing(board, place, (ow_ref.at[:, :half_cols], ow_ref.at[:, half_cols:]), (owa, owb))
    share_w = PlaneShare(board, place, (wq, wkv))
    quarter = (share_w.rows(0, 0), share_w.rows(1, 0))
    wring = ZRing(board, place, (dq_ref.at[quarter[0]], dkv_ref.at[quarter[1]]), (wq, wkv),
                  rows=quarter)
    facing = (share_w.rows(0, 2), share_w.rows(1, 2))
    oring = ZRing(board, place, (dq_ref.at[facing[0]], dkv_ref.at[facing[1]]), (wq, wkv),
                  rows=facing)
    lring = ZRing(board, place, (lk.at[place.t], lq.at[place.t]), (lk, lq), by_device=True)

    mark("a_greet")
    greet([place.sp_peer(k) for k in range(1, 16)] + [place.tp_peer(k) for k in range(1, 16)])

    mark("b_mod")
    wring.begin()
    oring.begin()
    board.send(lat_d2d, lat_ref, latsib, place.sibling())

    def silu(ref):
        rows = lax.broadcasted_iota(jnp.int32, (16, 128), 0)
        v = jnp.sum(jnp.where(rows == place.s, ref[...].astype(F32), 0.0), axis=0, keepdims=True)
        return v / (1.0 + jnp.exp(-v))

    act = jnp.concatenate(
        [silu(cond_ref), silu(condc_ref), jnp.zeros((14, 128), F32)],
        axis=0).astype(BF)
    terms = [jnp.dot(act, mw_ref[r], preferred_element_type=F32) for r in range(3)]
    modp[place.s] = jnp.concatenate(
        [terms[0][0:1], terms[1][0:1], terms[2][0:1], terms[0][1:2], terms[1][1:2],
         jnp.zeros((3, 128), F32)], axis=0)
    for k in range(1, 16):
        board.send(modp_base + k, modp.at[place.s], modp.at[place.s], place.sp_peer(k))

    mark("c_local")
    wq[place.z] = dq_ref[...]
    wkv[place.z] = dkv_ref[...]
    owa[place.z] = ow_ref[:, :half_cols]
    owb[place.z] = ow_ref[:, half_cols:]
    wk[...] = jnp.zeros(wk.shape, BF)
    wk[0:NOPE, 0:512] = upk_ref[...]
    wk[HEAD:HEAD + VDIM, 0:512] = upv_ref[...]
    unit = (lax.broadcasted_iota(jnp.int32, (ROPE, 128), 0)
            == lax.broadcasted_iota(jnp.int32, (ROPE, 128), 1))
    wk[NOPE:HEAD, 512:640] = jnp.where(unit, 1.0, 0.0).astype(BF)

    def inverse(ref):
        rows = ref[...].astype(F32)
        return lax.rsqrt(jnp.mean(rows * rows, axis=-1, keepdims=True) + epsilon)

    inv_own = inverse(lat_ref)
    inv_ctx = inverse(context_ref)

    mark("d_modwait")
    def from_ring(dist):
        for part in (0, 1):
            if dist == 4:
                wring.take(1 if part == 0 else -1, 4, part)
                share_w.send(4, part)
                continue
            for way in (1, -1):
                wring.take(way, dist, part)
                share_w.send(way * dist, part)

    def facing_ring(dist):
        for part in (0, 1):
            for way in ((1 if part == 0 else -1,) if dist == 4 else (1, -1)):
                oring.take(way, dist, part)

    from_ring(1)
    facing_ring(1)
    for k in range(1, 16):
        board.arrived(modp_base + k, modp.at[(place.s - k + 16) % 16], place.sp_peer(16 - k))
    modf[place.t] = jnp.sum(modp[...], axis=0)
    for k in range(1, 16):
        board.send(modf_base + k, modf.at[place.t], modf.at[place.t], place.tp_peer(k))

    board.arrived(lat_d2d, latsib, place.sibling())
    inv_sib = inverse(latsib)
    from_ring(2)
    facing_ring(2)
    mark("e_modfwait")
    for k in range(1, 16):
        board.arrived(modf_base + k, modf.at[(place.t - k + 16) % 16], place.tp_peer(16 - k))

    mark("f_norm")
    norm_gain = ng_ref[...].astype(F32)
    for k in range(16):
        cols = slice(k * 128, (k + 1) * 128)
        gain = norm_gain[k:k + 1]
        shift, scale = modf[k, 0:1, :], modf[k, 1:2, :]
        own = lat_ref[:, cols].astype(F32) * inv_own * gain
        xn[k, 0:64] = (own * (1.0 + scale) + shift).astype(BF)
        sib = latsib[:, cols].astype(F32) * inv_sib * gain
        xn[k, 96:160] = (sib * (1.0 + scale) + shift).astype(BF)
        ctx = context_ref[:, cols].astype(F32) * inv_ctx * gain
        xn[k, 64:96] = (ctx * (1.0 + modf[k, 4:5, :]) + modf[k, 3:4, :]).astype(BF)

    def add_product(at, part):
        rows = xn[2 * at + place.c]
        if part == 0:
            uq[...] += jnp.dot(rows, wq[at], preferred_element_type=F32)
        else:
            ukv[...] += jnp.dot(rows, wkv[at], preferred_element_type=F32)

    uq[...] = jnp.dot(xn[place.t], wq[place.z], preferred_element_type=F32)
    ukv[...] = jnp.dot(xn[place.t], wkv[place.z], preferred_element_type=F32)
    contract = (((1,), (1,)), ((), ()))
    rope = jnp.zeros((96, ROPE), F32)
    for k in range(16):
        rope = rope + lax.dot_general(xn[k, 0:96], rw_ref[:, k * 128:(k + 1) * 128], contract,
                                      preferred_element_type=F32)
    rope = rope.astype(BF).astype(F32)
    mark("g_wring")
    def finish_chip(dist):
        for part in (0, 1):
            for d in ((4,) if dist == 4 else (dist, -dist)):
                share_w.arrived(d, part)
                add_product((place.z - d + 16) % 8, part)

    from_ring(3)
    finish_chip(1)
    facing_ring(3)
    finish_chip(2)
    from_ring(4)
    finish_chip(3)
    facing_ring(4)
    finish_chip(4)

    mark("h_d2dpart")
    board.send(part_base + 1, ukv.at[64:160], skv, place.sibling())
    board.send(part_base, uq.at[96:160], sq, place.sibling())

    def latent_of(total, gain_ref):
        gain = gain_ref[...].astype(F32)
        gain = jnp.concatenate([gain[k:k + 1] for k in range(gain.shape[0])], axis=1)
        return (total * lax.rsqrt(jnp.mean(total * total, axis=-1, keepdims=True) + epsilon)
                * gain).astype(BF)

    board.arrived(part_base + 1, skv, place.sibling())
    lk[place.t, :, 0:512] = latent_of(ukv[0:64] + skv[32:96], kvlg_ref)
    lk[place.t, :, 512:640] = jnp.concatenate(
        [rope[0:64], jnp.zeros((64, 96), F32)], axis=1).astype(BF)
    def share(number, ref):
        board.send(share_base + number, ref, ref, place.sibling())

    lring.begin_part(0)
    share(0, lk.at[place.t])
    board.arrived(part_base, sq, place.sibling())
    lq[place.t] = latent_of(uq[0:64] + sq[...], qlg_ref)
    lring.begin_part(1)
    share(1, lq.at[place.t])

    mark("i_ctx")
    ctx_kv = latent_of(ukv[64:96] + skv[0:32], kvlg_ref)
    ctx_k = lax.dot_general(ctx_kv, upk_ref[...], contract, preferred_element_type=F32)
    ctx_v = lax.dot_general(ctx_kv, upv_ref[...], contract, preferred_element_type=F32)
    ctx_u = jnp.concatenate([ctx_k, rope[64:96]], axis=1)
    ctx_n = ctx_u * lax.rsqrt(jnp.mean(ctx_u * ctx_u, axis=-1, keepdims=True) + epsilon)
    ctx_n = ctx_n * kg_ref[...]
    cbuf[place.s] = jnp.concatenate(
        [ctx_n, jnp.zeros((CTX_DEV, 128 - HEAD), F32), ctx_v,
         jnp.zeros((CTX_DEV, 128 - VDIM), F32)], axis=1).astype(BF)
    for k in range(1, 16):
        board.send(ctx_base + k, cbuf.at[place.s], cbuf.at[place.s], place.sp_peer(k))

    base = base_ref[pl.ds(pl.multiple_of(place.s * 16, 16), 16)]
    base_cos, base_sin = base[0:8, 0:1], base[8:16, 0:1]
    rt[0:8] = tab_ref[0:8] * base_cos - tab_ref[8:16] * base_sin
    rt[8:16] = tab_ref[8:16] * base_cos + tab_ref[0:8] * base_sin
    rt[16:32] = tab_ref[16:32]

    def column(gain_ref):
        row = jnp.concatenate([gain_ref[...], jnp.zeros((1, 128 - HEAD), F32)], axis=1)
        return jnp.broadcast_to(row, (128, 128)).T[0:HEAD, 0:1]

    def turned(u, gain, cols):
        row_cos, row_sin = rt[0:8, cols], rt[8:16, cols]
        col_cos, col_sin = rt[16:24, cols], rt[24:32, cols]
        normal = u * lax.rsqrt(jnp.mean(u * u, axis=0, keepdims=True) + epsilon) * gain
        a, b, c, d = (normal[NOPE + 8 * n:NOPE + 8 * n + 8] for n in range(4))
        return jnp.concatenate(
            [normal[0:NOPE], a * row_cos - b * row_sin, b * row_cos + a * row_sin,
             c * col_cos - d * col_sin, d * col_cos + c * col_sin], axis=0)

    query_gain, key_gain = column(qg_ref), column(kg_ref)

    def finish():
        wring.drain()
        oring.drain()
        share_w.drain()
        lring.drain()
        board.sent(lat_d2d, lat_ref, place.sibling())
        for k in range(1, 16):
            board.sent(modp_base + k, modp.at[place.s], place.sp_peer(k))
            board.sent(modf_base + k, modf.at[place.t], place.tp_peer(k))
        board.sent(part_base, uq.at[96:160], place.sibling())
        board.sent(part_base + 1, ukv.at[64:160], place.sibling())
        share_sizes = [0, 1] + [item[2] for item in l_items]
        for n, part in enumerate(share_sizes):
            board.sent(share_base + n, (lk, lq)[part].at[0], place.sibling())

    def kv_ref(key):
        return quarter_ref(kvb, SLOT[unit_of(key)], key[1], key[4])

    def kv_send(key, src):
        axis, step, _ = ITEMS[key]
        board.send(kv_base + ITEM_INDEX[key], src, kv_ref(key), place.plane(axis, step))

    def kv_begin(h):
        for key in own_keys(ITEMS, h):
            kv_send(key, kvb.at[SLOT[(h, 0, 0)], key[1]])

    def kv_take(key):
        axis, step, _ = ITEMS[key]
        board.arrived(kv_base + ITEM_INDEX[key], kv_ref(key), place.plane(axis, -step))
        for other in ITEM_ORDER:
            if ITEMS[other][2] == key:
                kv_send(other, quarter_ref(kvb, SLOT[unit_of(key)], key[1], other[4]))

    mark("j_lring")
    l_items = lring.items()
    other = 1 - place.c

    def ring_take(way, dist, part):
        lring.take(way, dist, part)
        share(2 + l_items.index((way, dist, part)), lring.slot(way, dist, part))

    def chip(dist, part):
        at = (place.z - dist + 16) % 8
        if dist == 0:
            number = part
        elif dist == 4:
            number = 2 + l_items.index((1 if part == 0 else -1, 4, part))
        else:
            number = 2 + l_items.index((1 if dist > 0 else -1, abs(dist), part))
        buf = (lk, lq)[part]
        board.arrived(share_base + number, buf.at[at * 2 + other], place.sibling())
        cols = pl.ds(pl.multiple_of(at * 128, 128), 128)
        return buf[pl.ds(at * 2, 2)].reshape(128, buf.shape[2]), cols

    def chip_keys(dist, h, n):
        rows, cols = chip(dist, 0)
        kv = lax.dot_general(wk[...], rows, contract, preferred_element_type=F32)
        kv = jnp.concatenate([turned(kv[0:HEAD], key_gain, cols), kv[HEAD:HEAD + VDIM]], axis=0)
        kvb[SLOT[(h, 0, 0)], n // 2, :, (n % 2) * 128:(n % 2) * 128 + 128] = kv.astype(BF)

    def chip_queries(dist):
        rows, cols = chip(dist, 1)
        u = lax.dot_general(upq_ref[...], rows, contract, preferred_element_type=F32)
        qt[0:HEAD, cols] = turned(u, query_gain, cols).astype(BF)

    qt[HEAD:128] = jnp.zeros((128 - HEAD, 1024), BF)
    ring_take(1, 1, 0)
    ring_take(-1, 1, 0)
    chip_keys(0, 0, 0)
    ring_take(1, 1, 1)
    ring_take(-1, 1, 1)
    chip_keys(1, 0, 1)
    chip_keys(-1, 0, 2)
    ring_take(1, 2, 0)
    ring_take(-1, 2, 0)
    chip_queries(0)
    chip_keys(2, 0, 3)
    mark("k_h0")
    kv_begin(0)
    ring_take(1, 2, 1)
    ring_take(-1, 2, 1)
    chip_queries(1)
    chip_queries(-1)
    ring_take(1, 3, 0)
    ring_take(-1, 3, 0)
    chip_keys(-2, 1, 0)
    chip_queries(2)
    for key in EARLY[0]:
        kv_take(key)
    ring_take(1, 3, 1)
    ring_take(-1, 3, 1)
    ring.begin()
    chip_keys(3, 1, 1)
    chip_keys(-3, 1, 2)
    chip_queries(-2)
    mark("l_early")
    for key in EARLY[1]:
        kv_take(key)
    mark("l_h1")
    ring_take(1, 4, 0)
    chip_keys(4, 1, 3)
    kv_begin(1)
    mark("l_q")
    chip_queries(3)
    chip_queries(-3)
    for key in EARLY[2]:
        kv_take(key)
    ring_take(-1, 4, 1)
    chip_queries(4)

    def ctx_unit():
        for k in range(1, 16):
            board.arrived(ctx_base + k, cbuf.at[(place.s - k + 16) % 16], place.sp_peer(16 - k))
        turned = cbuf[...].reshape(512, 256).astype(F32).T.astype(BF)
        for q in (0, 1):
            kvb[CTX_SLOT, q, 0:HEAD, :] = turned[0:HEAD, q * 256:(q + 1) * 256]
            kvb[CTX_SLOT, q, HEAD:HEAD + VDIM, :] = turned[128:128 + VDIM, q * 256:(q + 1) * 256]

    mark("m_init")
    m_ref[...] = jnp.full(m_ref.shape, -jnp.inf, F32)
    l_ref[...] = jnp.zeros(l_ref.shape, F32)
    acc[...] = jnp.zeros(acc.shape, F32)

    def products(slot, s_ref, mb_ref):
        for q in (0, 1):
            keys = kvb[slot, q, 0:128, :].T
            for n in range(4):
                cols = slice(n * 256, (n + 1) * 256)
                scores = jnp.dot(keys, qt[:, cols], preferred_element_type=F32)
                s_ref[q * 256:(q + 1) * 256, cols] = scores
                top = jnp.max(scores, axis=0, keepdims=True)
                mb_ref[:, cols] = top if q == 0 else jnp.maximum(mb_ref[:, cols], top)

    ones = jnp.ones((16, 256), BF)

    def absorb(slot, s_ref, mb_ref, bias):
        values = [jnp.concatenate([kvb[slot, q, HEAD:HEAD + VDIM, :], ones], axis=0)
                  for q in (0, 1)]
        for n in range(4):
            cols = slice(n * 256, (n + 1) * 256)
            old = m_ref[:, cols]
            top = mb_ref[:, cols] * SCALE2
            if bias is not None:
                top = top + bias
            new = jnp.maximum(old, top)
            m_ref[:, cols] = new
            factor = jnp.exp2(old - new)
            less = new if bias is None else new - bias
            weights = jnp.exp2(s_ref[:, cols] * SCALE2 - less)
            rounded = weights.astype(BF)
            summed = jnp.dot(values[0], rounded[:256], preferred_element_type=F32)
            summed = summed + jnp.dot(values[1], rounded[256:], preferred_element_type=F32)
            l_ref[:, cols] = l_ref[:, cols] * factor + summed[VDIM:VDIM + 1]
            acc[:, cols] = acc[:, cols] * factor + summed[:VDIM]

    ring_items = ring.items()
    ring_plan = [[] for _ in range(17)]
    for n, item in enumerate(ring_items):
        ring_plan[16 if n >= 12 else 1 + n].append(item)

    def actions(n):
        for key in PLAN[n]:
            kv_take(key)
        for item in ring_plan[n]:
            ring.take(*item)

    mark("n_prolog")
    actions(0)
    products(0, s_a, mb_a)
    for i in range(16):
        mark(f"o{i:02d}a")
        actions(i + 1)
        if i == 15:
            ctx_unit()
        mark(f"o{i:02d}b")
        products(2 * i + 1, s_b, mb_b)
        absorb(2 * i, s_a, mb_a, None)
        products(2 * i + 2, s_a, mb_a)
        absorb(2 * i + 1, s_b, mb_b, None)
    mark("p_last")
    bias = (bias_ref[0, 0] + math.log(TOK_DEV / CTX_DEV)) * LOG2E
    absorb(CTX_SLOT, s_a, mb_a, bias)

    mark("q_a2a")
    for k in range(8):
        cols = slice(k * 128, (k + 1) * 128)
        att[k] = (acc[:, cols] / l_ref[:, cols]).astype(BF)
    for k in range(1, 8):
        board.send(a2a_base + k, att.at[(place.z + k) % 8], attb.at[place.z], place.ring(k))
    attb[place.z] = att[place.z]
    for k in range(1, 8):
        board.arrived(a2a_base + k, attb.at[(place.z - k + 8) % 8], place.ring(-k))
    mark("r_out")
    rows = attb[...].reshape(8 * VDIM, 128).astype(F32).T.astype(BF)
    for n, weight in enumerate((owa, owb)):
        part_ref[:, n * half_cols:(n + 1) * half_cols] = jnp.dot(
            rows, weight[...].reshape(8 * VDIM, half_cols), preferred_element_type=F32)
    away = part_ref.at[pl.ds(pl.multiple_of(64 * (1 - place.c), 64), 64)]
    mark("s_d2d")
    board.send(d2d, away, sib_ref, place.sibling())
    board.arrived(d2d, sib_ref, place.sibling())
    gates = jnp.concatenate([modf[k, 2:3, :] for k in range(16)], axis=1)
    mine = part_ref[pl.ds(pl.multiple_of(64 * place.c, 64), 64)]
    projected = mine + sib_ref[...]
    out_ref[...] = (lat_ref[...].astype(F32) + gates * projected).astype(BF)

    mark("t_drain")
    board.sent(d2d, away, place.sibling())
    for k in range(1, 8):
        board.sent(a2a_base + k, att.at[(place.z + k) % 8], place.ring(k))
    for k in range(1, 16):
        board.sent(ctx_base + k, cbuf.at[place.s], place.sp_peer(k))
    ring.drain()
    finish()
    for key in ITEM_ORDER:
        axis, step, _ = ITEMS[key]
        src = quarter_ref(kvb, 0, 0, key[4])
        board.sent(kv_base + ITEM_INDEX[key], src, place.plane(axis, step))
    mark(None)


def rotation_tables():
    frequency = np.power(np.float32(theta), -np.arange(8, dtype=np.float32) / np.float32(8))
    frequency = frequency.astype(np.float32).astype(np.float64)[:, None]
    token = np.arange(1024)[None, :]
    row, col = frequency * (token // GRID_W), frequency * (token % GRID_W)
    table = np.concatenate([np.cos(row), np.sin(row), np.cos(col), np.sin(col)])
    first = frequency * (np.arange(16)[None, :] * 16)
    base = np.stack([np.cos(first), np.sin(first)]).reshape(16, 16).T.reshape(256, 1)
    base = np.broadcast_to(base, (256, 128))
    return base.astype(np.float32), table.astype(np.float32)


def shards(
    latent,
    context,
    cond,
    cond_context,
    mod_weight,
    norm_gain,
    down_q,
    down_kv,
    rope_weight,
    qlat_gain,
    kvlat_gain,
    up_query,
    up_key,
    up_value,
    query_gain,
    key_gain,
    context_bias,
    out_weight,
):
    vmem = pl.BlockSpec(memory_space=pltpu.VMEM)
    smem = pl.BlockSpec(memory_space=pltpu.SMEM)
    copies = len(ITEM_ORDER) + 16 + 8 + 2 + 32 + 2 + 16 + 4 * 16 + 28
    base, table = rotation_tables()
    row = lambda v: v.reshape(1, -1)
    fold = lambda v: v.reshape(-1, 128)
    return pl.pallas_call(
        whole_kernel,
        out_shape=jax.ShapeDtypeStruct((64, D), BF),
        in_specs=[vmem] * 16 + [smem] + [vmem] * 3,
        out_specs=vmem,
        scratch_shapes=[
            pltpu.VMEM((8, 128, 768), BF),
            pltpu.VMEM((8, 128, 512), BF),
            pltpu.VMEM((64, D), BF),
            pltpu.VMEM((16, 8, 128), F32),
            pltpu.VMEM((16, 8, 128), F32),
            pltpu.VMEM((16, 160, 128), BF),
            pltpu.VMEM((160, 768), F32),
            pltpu.VMEM((160, 512), F32),
            pltpu.VMEM((64, 768), F32),
            pltpu.VMEM((96, 512), F32),
            pltpu.VMEM((16, 64, 768), BF),
            pltpu.VMEM((16, 64, 640), BF),
            pltpu.VMEM((160, 640), BF),
            pltpu.VMEM((ROPE, 1024), F32),
            pltpu.VMEM((128, 1024), BF),
            pltpu.VMEM((N_UNITS, 2, HEAD + VDIM, 256), BF),
            pltpu.VMEM((16, CTX_DEV, 256), BF),
            pltpu.VMEM((8, 64, D // 2), BF),
            pltpu.VMEM((8, 64, D // 2), BF),
            pltpu.VMEM((512, 1024), F32),
            pltpu.VMEM((512, 1024), F32),
            pltpu.VMEM((1, 1024), F32),
            pltpu.VMEM((1, 1024), F32),
            pltpu.VMEM((1, 1024), F32),
            pltpu.VMEM((1, 1024), F32),
            pltpu.VMEM((VDIM, 1024), F32),
            pltpu.VMEM((8, VDIM, 128), BF),
            pltpu.VMEM((8, VDIM, 128), BF),
            pltpu.VMEM((128, D), F32),
            pltpu.VMEM((64, D), F32),
            pltpu.SemaphoreType.DMA((copies,)),
            pltpu.SemaphoreType.DMA((copies,)),
        ],
        compiler_params=pltpu.CompilerParams(collective_id=0, has_side_effects=True,
                                             vmem_limit_bytes=56 * 1024 * 1024),
        name="whole",
    )(latent, context, fold(cond), fold(cond_context), mod_weight, fold(norm_gain), down_q, down_kv,
      rope_weight.T, fold(qlat_gain), fold(kvlat_gain), up_query.T, up_key.T, up_value.T, row(query_gain),
      row(key_gain), context_bias.reshape(1, 1), out_weight, jnp.asarray(base),
      jnp.asarray(table))


def solution(mesh):
    placed = (
        P(SP_TP, None),
        P("sp", None),
        P(),
        P(),
        P(None, "sp", "tp"),
        P(),
        P("tp", None),
        P("tp", None),
        P(),
        P(),
        P(),
        P(None, "tp"),
        P(None, "tp"),
        P(None, "tp"),
        P(),
        P(),
        P("tp"),
        P("tp", None),
    )
    return jax.shard_map(
        shards, mesh=mesh, in_specs=placed, out_specs=P(SP_TP, None), check_vma=False
    )
```

```python
import math

import jax
import jax.numpy as jnp
import numpy as np
from jax import lax
from jax.experimental import pallas as pl
from jax.experimental.pallas import tpu as pltpu
from jax.sharding import PartitionSpec as P

NOPE = 64
ROPE = 32
HEAD = NOPE + ROPE
VDIM = 64
GRID_W = 64
TOK_DEV = 1024
CTX_DEV = 32
D = 2048
SP_TP = ("sp", "tp")
BF = jnp.bfloat16
F32 = jnp.float32

epsilon = 1e-06
theta = 10000.0
SCALE2 = math.log2(math.e) * HEAD ** (-0.5)
LOG2E = math.log2(math.e)


def exchange_items():
    items = {}
    for h in (0, 1):
        for q in (0, 1):
            def add(da, db, part, axis, step, trigger):
                names = ("x", "y") if q == 0 else ("y", "x")
                trigger = None if trigger is None else (h, q) + trigger
                items[(h, q, da, db, part)] = (names[axis], step, trigger)
            add(-1, 0, "U", 0, 1, None)
            add(1, 0, "U", 0, -1, None)
            add(2, 0, 0, 0, 1, (-1, 0, "U"))
            add(2, 0, 1, 0, -1, (1, 0, "U"))
            for da in (0, -1, 1):
                trigger = None if da == 0 else (da, 0, "U")
                add(da, -1, "U", 1, 1, trigger)
                add(da, 1, "U", 1, -1, trigger)
                add(da, 2, 0, 1, 1, (da, -1, "U"))
                add(da, 2, 1, 1, -1, (da, 1, "U"))
            for part in (0, 1):
                add(2, -1, part, 1, 1, (2, 0, part))
                add(2, 1, part, 1, -1, (2, 0, part))
            add(2, 2, 0, 1, 1, (2, -1, 0))
            add(2, 2, 1, 1, -1, (2, 1, 1))
    return items


def unit_of(key):
    h, q, da, db, _ = key
    return (h, da, db) if q == 0 else (h, db, da)


RELEASE = (9.0, 17.4)
LOOKS = (13.2, 16.0, 18.8)
LOOP_AT = 20.2
STEP = 0.79
UNIT, LATENCY = 1.85, 2.0


def plan_exchange(items):
    free, arrive = {}, {}
    taken = []

    def send(key, at):
        axis, step, _ = items[key]
        begin = max(at, free.get((axis, step), 0.0))
        free[(axis, step)] = begin + (UNIT if key[4] == "U" else UNIT / 2)
        arrive[key] = free[(axis, step)] + LATENCY

    def begin_half(h, at):
        for key in own_keys(items, h):
            send(key, at)

    def rank(key):
        return (round(arrive[key], 1), 0 if key[3] == 0 else 1, str(key))

    def take(now):
        got = []
        while True:
            here = sorted((k for k in arrive if k not in taken and arrive[k] <= now), key=rank)
            if not here:
                return got
            key = here[0]
            taken.append(key)
            got.append(key)
            for other in items:
                if items[other][2] == key:
                    send(other, now)

    begin_half(0, RELEASE[0])
    early = [take(LOOKS[0]), take(LOOKS[1])]
    begin_half(1, RELEASE[1])
    early.append(take(LOOKS[2]))
    now = LOOP_AT
    units = [(0, 0, 0), (1, 0, 0)]
    every = sorted({unit_of(k) for k in items})

    def come(u):
        return max(arrive[k] for k in items if unit_of(k) == u)

    def ready():
        done = [u for u in every if u not in units
                and all(k in taken for k in items if unit_of(k) == u)]
        return sorted(done, key=lambda u: (come(u), str(u)))

    plan = [take(now)]
    for n in range(1, len(every) + 3, 2):
        got = take(now)
        while len(units) < min(n + 2, len(every) + 2):
            found = ready()
            if found:
                units.append(found[0])
                continue
            now = min(arrive[k] for k in arrive if k not in taken)
            got = got + take(now)
        plan.append(got)
        now += 2 * STEP
    return early, plan, units, now


def own_keys(items, h):
    keys = [k for k in items if items[k][2] is None and k[0] == h]
    return sorted(keys, key=lambda k: 0 if items[k][0] == ("x", "y")[k[1]] else 1)


ITEMS = exchange_items()
EARLY, PLAN, UNITS, PLAN_END = plan_exchange(ITEMS)
ITEM_ORDER = list(ITEMS)
ITEM_INDEX = {k: n for n, k in enumerate(ITEM_ORDER)}
SLOT = {u: n for n, u in enumerate(UNITS)}
N_UNITS = len(UNITS) + 1
CTX_SLOT = len(UNITS)


def mark(name):
    pass


class Board:
    def __init__(self, sends, recvs):
        self.sends, self.recvs, self.count, self.started = sends, recvs, 0, []

    def take(self, n=1):
        first = self.count
        self.count += n
        return first

    def send(self, number, src, dst, device):
        copy = pltpu.make_async_remote_copy(
            src_ref=src, dst_ref=dst, send_sem=self.sends.at[number],
            recv_sem=self.recvs.at[number], device_id=device,
            device_id_type=pl.DeviceIdType.MESH)
        copy.start()

    def arrived(self, number, dst, device):
        pltpu.make_async_remote_copy(
            src_ref=dst, dst_ref=dst, send_sem=self.sends.at[number],
            recv_sem=self.recvs.at[number], device_id=device,
            device_id_type=pl.DeviceIdType.MESH).wait_recv()

    def sent(self, number, src, device):
        pltpu.make_async_remote_copy(
            src_ref=src, dst_ref=src, send_sem=self.sends.at[number],
            recv_sem=self.recvs.at[number], device_id=device,
            device_id_type=pl.DeviceIdType.MESH).wait_send()


CHIPS = (1, -1, 2, -2, 3, -3, 4)


class PlaneShare:
    def __init__(self, board, place, bufs):
        self.board, self.place, self.bufs = board, place, bufs
        self.base = board.take(len(CHIPS) * 4)

    def rows(self, part, offset):
        at = ((self.place.x, self.place.y)[part] + offset + 4) % 4 * 32
        return pl.ds(pl.multiple_of(at, 32), 32)

    def view(self, dist, part, offset):
        return self.bufs[part].at[(self.place.z - dist + 16) % 8, self.rows(part, offset)]

    def number(self, dist, part, kind):
        return self.base + (CHIPS.index(dist) * 2 + part) * 2 + kind

    def device(self, part, step):
        return self.place.plane(("x", "y")[part], step)

    def send(self, dist, part):
        own = self.view(dist, part, 0)
        self.board.send(self.number(dist, part, 0), own, own, self.device(part, 1))
        self.board.send(self.number(dist, part, 1), own, own, self.device(part, -1))

    def arrived(self, dist, part):
        for kind, step in ((0, 1), (1, -1)):
            self.board.arrived(self.number(dist, part, kind), self.view(dist, part, -step),
                               self.device(part, -step))

    def drain(self):
        for dist in CHIPS:
            for part in (0, 1):
                for kind, step in ((0, 1), (1, -1)):
                    self.board.sent(self.number(dist, part, kind), self.view(dist, part, 0),
                                    self.device(part, step))


class Place:
    def __init__(self):
        self.s = lax.axis_index("sp")
        self.t = lax.axis_index("tp")
        self.y, self.x = self.s // 4, self.s % 4
        self.z, self.c = self.t // 2, self.t % 2

    def plane(self, axis, step):
        y, x = self.y, self.x
        if axis == "x":
            x = (x + step + 4) % 4
        else:
            y = (y + step + 4) % 4
        return {"sp": y * 4 + x, "tp": self.t}

    def sp_peer(self, k):
        return {"sp": (self.s + k) % 16, "tp": self.t}

    def tp_peer(self, k):
        return {"sp": self.s, "tp": (self.t + k) % 16}

    def ring(self, step):
        return {"sp": self.s, "tp": ((self.z + step + 8) % 8) * 2 + self.c}

    def sibling(self):
        return {"sp": self.s, "tp": self.z * 2 + 1 - self.c}


def greet(devices):
    barrier = pltpu.get_barrier_semaphore()
    for device in devices:
        pl.semaphore_signal(barrier, inc=1, device_id=device,
                            device_id_type=pl.DeviceIdType.MESH)
    pl.semaphore_wait(barrier, len(devices))


class ZRing:
    def __init__(self, board, place, own, bufs, by_device=False, rows=None):
        self.rows = rows
        self.board, self.place, self.own, self.bufs = board, place, own, bufs
        self.by_device = by_device
        self.base = board.take(16)

    def number(self, way, dist, part):
        return self.base + (0 if way == 1 else 8) + (dist - 1) * 2 + part

    def slot(self, way, dist, part):
        return self.view(part, way * dist)

    def view(self, part, back):
        if self.rows is None:
            return self.bufs[part].at[self.index(back)]
        return self.bufs[part].at[self.index(back), self.rows[part]]

    def index(self, back):
        at = (self.place.z - back + 16) % 8
        return at * 2 + self.place.c if self.by_device else at

    def begin(self):
        for part in (0, 1):
            self.begin_part(part)

    def begin_part(self, part):
        for way in (1, -1):
            self.board.send(self.number(way, 1, part), self.own[part],
                            self.view(part, 0), self.place.ring(way))

    def take(self, way, dist, part):
        here = self.slot(way, dist, part)
        self.board.arrived(self.number(way, dist, part), here, self.place.ring(-way))
        if dist < 3 or (dist == 3 and part == (0 if way == 1 else 1)):
            self.board.send(self.number(way, dist + 1, part), here, here, self.place.ring(way))

    def items(self):
        out = []
        for dist in (1, 2, 3):
            for part in (0, 1):
                for way in (1, -1):
                    out.append((way, dist, part))
        out.append((1, 4, 0))
        out.append((-1, 4, 1))
        return out

    def drain(self):
        for part in (0, 1):
            for way in (1, -1):
                self.board.sent(self.number(way, 1, part), self.own[part], self.place.ring(way))
        for way, dist, part in self.items():
            if dist > 1:
                here = self.slot(way, dist - 1, part)
                self.board.sent(self.number(way, dist, part), here, self.place.ring(way))


def quarter_ref(buf, slot, quarter, part):
    if part == "U":
        return buf.at[slot, quarter]
    return buf.at[slot, quarter, :, 128 * part:128 * part + 128]


def whole_kernel(lat_ref, context_ref, cond_ref, condc_ref, mw_ref, ng_ref, dq_ref, dkv_ref,
                 rw_ref, qlg_ref, kvlg_ref, upq_ref, upk_ref, upv_ref, qg_ref, kg_ref, bias_ref,
                 ow_ref, base_ref, tab_ref, out_ref,
                 wq, wkv, latsib, modp, modf, xn, uq, ukv, sq, skv, lq, lk, wk, rt,
                 qt, kvb, cbuf, owa, owb, s_a, s_b, mb_a, mb_b, m_ref, l_ref, acc, att, attb,
                 part_ref, sib_ref, sends, recvs):
    place = Place()
    board = Board(sends, recvs)
    kv_base = board.take(len(ITEM_ORDER))
    ctx_base = board.take(16)
    a2a_base = board.take(8)
    d2d = board.take(2)
    lat_d2d = board.take(1)
    modp_base = board.take(16)
    modf_base = board.take(16)
    part_base = board.take(2)
    share_base = board.take(16)
    half_cols = D // 2
    ring = ZRing(board, place, (ow_ref.at[:, :half_cols], ow_ref.at[:, half_cols:]), (owa, owb))
    share_w = PlaneShare(board, place, (wq, wkv))
    quarter = (share_w.rows(0, 0), share_w.rows(1, 0))
    wring = ZRing(board, place, (dq_ref.at[quarter[0]], dkv_ref.at[quarter[1]]), (wq, wkv),
                  rows=quarter)
    facing = (share_w.rows(0, 2), share_w.rows(1, 2))
    oring = ZRing(board, place, (dq_ref.at[facing[0]], dkv_ref.at[facing[1]]), (wq, wkv),
                  rows=facing)
    lring = ZRing(board, place, (lk.at[place.t], lq.at[place.t]), (lk, lq), by_device=True)

    mark("a_greet")
    greet([place.sp_peer(k) for k in range(1, 16)] + [place.tp_peer(k) for k in range(1, 16)])

    mark("b_mod")
    wring.begin()
    oring.begin()
    board.send(lat_d2d, lat_ref, latsib, place.sibling())

    def silu(ref):
        rows = lax.broadcasted_iota(jnp.int32, (16, 128), 0)
        v = jnp.sum(jnp.where(rows == place.s, ref[...].astype(F32), 0.0), axis=0, keepdims=True)
        return v / (1.0 + jnp.exp(-v))

    act = jnp.concatenate(
        [silu(cond_ref), silu(condc_ref), jnp.zeros((14, 128), F32)],
        axis=0).astype(BF)
    terms = [jnp.dot(act, mw_ref[r], preferred_element_type=F32) for r in range(3)]
    modp[place.s] = jnp.concatenate(
        [terms[0][0:1], terms[1][0:1], terms[2][0:1], terms[0][1:2], terms[1][1:2],
         jnp.zeros((3, 128), F32)], axis=0)
    for k in range(1, 16):
        board.send(modp_base + k, modp.at[place.s], modp.at[place.s], place.sp_peer(k))

    mark("c_local")
    wq[place.z] = dq_ref[...]
    wkv[place.z] = dkv_ref[...]
    owa[place.z] = ow_ref[:, :half_cols]
    owb[place.z] = ow_ref[:, half_cols:]
    wk[...] = jnp.zeros(wk.shape, BF)
    wk[0:NOPE, 0:512] = upk_ref[...]
    wk[HEAD:HEAD + VDIM, 0:512] = upv_ref[...]
    unit = (lax.broadcasted_iota(jnp.int32, (ROPE, 128), 0)
            == lax.broadcasted_iota(jnp.int32, (ROPE, 128), 1))
    wk[NOPE:HEAD, 512:640] = jnp.where(unit, 1.0, 0.0).astype(BF)

    def inverse(ref):
        rows = ref[...].astype(F32)
        return lax.rsqrt(jnp.mean(rows * rows, axis=-1, keepdims=True) + epsilon)

    inv_own = inverse(lat_ref)
    inv_ctx = inverse(context_ref)

    mark("d_modwait")
    def from_ring(dist):
        for part in (0, 1):
            if dist == 4:
                wring.take(1 if part == 0 else -1, 4, part)
                share_w.send(4, part)
                continue
            for way in (1, -1):
                wring.take(way, dist, part)
                share_w.send(way * dist, part)

    def facing_ring(dist):
        for part in (0, 1):
            for way in ((1 if part == 0 else -1,) if dist == 4 else (1, -1)):
                oring.take(way, dist, part)

    from_ring(1)
    facing_ring(1)
    for k in range(1, 16):
        board.arrived(modp_base + k, modp.at[(place.s - k + 16) % 16], place.sp_peer(16 - k))
    modf[place.t] = jnp.sum(modp[...], axis=0)
    for k in range(1, 16):
        board.send(modf_base + k, modf.at[place.t], modf.at[place.t], place.tp_peer(k))

    board.arrived(lat_d2d, latsib, place.sibling())
    inv_sib = inverse(latsib)
    from_ring(2)
    facing_ring(2)
    from_ring(3)
    facing_ring(3)
    mark("e_modfwait")
    for k in range(1, 16):
        board.arrived(modf_base + k, modf.at[(place.t - k + 16) % 16], place.tp_peer(16 - k))

    mark("f_norm")
    norm_gain = ng_ref[...].astype(F32)
    for k in range(16):
        cols = slice(k * 128, (k + 1) * 128)
        gain = norm_gain[k:k + 1]
        shift, scale = modf[k, 0:1, :], modf[k, 1:2, :]
        own = lat_ref[:, cols].astype(F32) * inv_own * gain
        xn[k, 0:64] = (own * (1.0 + scale) + shift).astype(BF)
        sib = latsib[:, cols].astype(F32) * inv_sib * gain
        xn[k, 96:160] = (sib * (1.0 + scale) + shift).astype(BF)
        ctx = context_ref[:, cols].astype(F32) * inv_ctx * gain
        xn[k, 64:96] = (ctx * (1.0 + modf[k, 4:5, :]) + modf[k, 3:4, :]).astype(BF)

    def add_product(at, part):
        rows = xn[2 * at + place.c]
        if part == 0:
            uq[...] += jnp.dot(rows, wq[at], preferred_element_type=F32)
        else:
            ukv[...] += jnp.dot(rows, wkv[at], preferred_element_type=F32)

    uq[...] = jnp.dot(xn[place.t], wq[place.z], preferred_element_type=F32)
    ukv[...] = jnp.dot(xn[place.t], wkv[place.z], preferred_element_type=F32)
    contract = (((1,), (1,)), ((), ()))
    rope = jnp.zeros((96, ROPE), F32)
    for k in range(16):
        rope = rope + lax.dot_general(xn[k, 0:96], rw_ref[:, k * 128:(k + 1) * 128], contract,
                                      preferred_element_type=F32)
    rope = rope.astype(BF).astype(F32)
    mark("g_wring")
    def finish_chip(dist):
        for part in (0, 1):
            for d in ((4,) if dist == 4 else (dist, -dist)):
                share_w.arrived(d, part)
                add_product((place.z - d + 16) % 8, part)

    finish_chip(1)
    from_ring(4)
    finish_chip(2)
    finish_chip(3)
    facing_ring(4)
    finish_chip(4)

    mark("h_d2dpart")
    board.send(part_base + 1, ukv.at[64:160], skv, place.sibling())
    board.send(part_base, uq.at[96:160], sq, place.sibling())

    def latent_of(total, gain_ref):
        gain = gain_ref[...].astype(F32)
        gain = jnp.concatenate([gain[k:k + 1] for k in range(gain.shape[0])], axis=1)
        return (total * lax.rsqrt(jnp.mean(total * total, axis=-1, keepdims=True) + epsilon)
                * gain).astype(BF)

    board.arrived(part_base + 1, skv, place.sibling())
    lk[place.t, :, 0:512] = latent_of(ukv[0:64] + skv[32:96], kvlg_ref)
    lk[place.t, :, 512:640] = jnp.concatenate(
        [rope[0:64], jnp.zeros((64, 96), F32)], axis=1).astype(BF)
    def share(number, ref):
        board.send(share_base + number, ref, ref, place.sibling())

    lring.begin_part(0)
    share(0, lk.at[place.t])
    board.arrived(part_base, sq, place.sibling())
    lq[place.t] = latent_of(uq[0:64] + sq[...], qlg_ref)
    lring.begin_part(1)
    share(1, lq.at[place.t])

    mark("i_ctx")
    ctx_kv = latent_of(ukv[64:96] + skv[0:32], kvlg_ref)
    ctx_k = lax.dot_general(ctx_kv, upk_ref[...], contract, preferred_element_type=F32)
    ctx_v = lax.dot_general(ctx_kv, upv_ref[...], contract, preferred_element_type=F32)
    ctx_u = jnp.concatenate([ctx_k, rope[64:96]], axis=1)
    ctx_n = ctx_u * lax.rsqrt(jnp.mean(ctx_u * ctx_u, axis=-1, keepdims=True) + epsilon)
    ctx_n = ctx_n * kg_ref[...]
    cbuf[place.s] = jnp.concatenate(
        [ctx_n, jnp.zeros((CTX_DEV, 128 - HEAD), F32), ctx_v,
         jnp.zeros((CTX_DEV, 128 - VDIM), F32)], axis=1).astype(BF)
    for k in range(1, 16):
        board.send(ctx_base + k, cbuf.at[place.s], cbuf.at[place.s], place.sp_peer(k))

    base = base_ref[pl.ds(pl.multiple_of(place.s * 16, 16), 16)]
    base_cos, base_sin = base[0:8, 0:1], base[8:16, 0:1]
    rt[0:8] = tab_ref[0:8] * base_cos - tab_ref[8:16] * base_sin
    rt[8:16] = tab_ref[8:16] * base_cos + tab_ref[0:8] * base_sin
    rt[16:32] = tab_ref[16:32]

    def column(gain_ref):
        row = jnp.concatenate([gain_ref[...], jnp.zeros((1, 128 - HEAD), F32)], axis=1)
        return jnp.broadcast_to(row, (128, 128)).T[0:HEAD, 0:1]

    def turned(u, gain, cols):
        row_cos, row_sin = rt[0:8, cols], rt[8:16, cols]
        col_cos, col_sin = rt[16:24, cols], rt[24:32, cols]
        normal = u * lax.rsqrt(jnp.mean(u * u, axis=0, keepdims=True) + epsilon) * gain
        a, b, c, d = (normal[NOPE + 8 * n:NOPE + 8 * n + 8] for n in range(4))
        return jnp.concatenate(
            [normal[0:NOPE], a * row_cos - b * row_sin, b * row_cos + a * row_sin,
             c * col_cos - d * col_sin, d * col_cos + c * col_sin], axis=0)

    query_gain, key_gain = column(qg_ref), column(kg_ref)

    def finish():
        wring.drain()
        oring.drain()
        share_w.drain()
        lring.drain()
        board.sent(lat_d2d, lat_ref, place.sibling())
        for k in range(1, 16):
            board.sent(modp_base + k, modp.at[place.s], place.sp_peer(k))
            board.sent(modf_base + k, modf.at[place.t], place.tp_peer(k))
        board.sent(part_base, uq.at[96:160], place.sibling())
        board.sent(part_base + 1, ukv.at[64:160], place.sibling())
        share_sizes = [0, 1] + [item[2] for item in l_items]
        for n, part in enumerate(share_sizes):
            board.sent(share_base + n, (lk, lq)[part].at[0], place.sibling())

    def kv_ref(key):
        return quarter_ref(kvb, SLOT[unit_of(key)], key[1], key[4])

    def kv_send(key, src):
        axis, step, _ = ITEMS[key]
        board.send(kv_base + ITEM_INDEX[key], src, kv_ref(key), place.plane(axis, step))

    def kv_begin(h):
        for key in own_keys(ITEMS, h):
            kv_send(key, kvb.at[SLOT[(h, 0, 0)], key[1]])

    def kv_take(key):
        axis, step, _ = ITEMS[key]
        board.arrived(kv_base + ITEM_INDEX[key], kv_ref(key), place.plane(axis, -step))
        for other in ITEM_ORDER:
            if ITEMS[other][2] == key:
                kv_send(other, quarter_ref(kvb, SLOT[unit_of(key)], key[1], other[4]))

    mark("j_lring")
    l_items = lring.items()
    other = 1 - place.c

    def ring_take(way, dist, part):
        lring.take(way, dist, part)
        share(2 + l_items.index((way, dist, part)), lring.slot(way, dist, part))

    def chip(dist, part):
        at = (place.z - dist + 16) % 8
        if dist == 0:
            number = part
        elif dist == 4:
            number = 2 + l_items.index((1 if part == 0 else -1, 4, part))
        else:
            number = 2 + l_items.index((1 if dist > 0 else -1, abs(dist), part))
        buf = (lk, lq)[part]
        board.arrived(share_base + number, buf.at[at * 2 + other], place.sibling())
        cols = pl.ds(pl.multiple_of(at * 128, 128), 128)
        return buf[pl.ds(at * 2, 2)].reshape(128, buf.shape[2]), cols

    def chip_keys(dist, h, n):
        rows, cols = chip(dist, 0)
        kv = lax.dot_general(wk[...], rows, contract, preferred_element_type=F32)
        kv = jnp.concatenate([turned(kv[0:HEAD], key_gain, cols), kv[HEAD:HEAD + VDIM]], axis=0)
        kvb[SLOT[(h, 0, 0)], n // 2, :, (n % 2) * 128:(n % 2) * 128 + 128] = kv.astype(BF)

    def chip_queries(dist):
        rows, cols = chip(dist, 1)
        u = lax.dot_general(upq_ref[...], rows, contract, preferred_element_type=F32)
        qt[0:HEAD, cols] = turned(u, query_gain, cols).astype(BF)

    qt[HEAD:128] = jnp.zeros((128 - HEAD, 1024), BF)
    ring_take(1, 1, 0)
    ring_take(-1, 1, 0)
    chip_keys(0, 0, 0)
    ring_take(1, 1, 1)
    ring_take(-1, 1, 1)
    chip_keys(1, 0, 1)
    chip_keys(-1, 0, 2)
    ring_take(1, 2, 0)
    ring_take(-1, 2, 0)
    chip_queries(0)
    chip_keys(2, 0, 3)
    mark("k_h0")
    kv_begin(0)
    ring_take(1, 2, 1)
    ring_take(-1, 2, 1)
    chip_queries(1)
    chip_queries(-1)
    ring_take(1, 3, 0)
    ring_take(-1, 3, 0)
    chip_keys(-2, 1, 0)
    chip_queries(2)
    for key in EARLY[0]:
        kv_take(key)
    ring_take(1, 3, 1)
    ring_take(-1, 3, 1)
    ring.begin()
    chip_keys(3, 1, 1)
    chip_keys(-3, 1, 2)
    chip_queries(-2)
    mark("l_early")
    for key in EARLY[1]:
        kv_take(key)
    mark("l_h1")
    ring_take(1, 4, 0)
    chip_keys(4, 1, 3)
    kv_begin(1)
    mark("l_q")
    chip_queries(3)
    chip_queries(-3)
    for key in EARLY[2]:
        kv_take(key)
    ring_take(-1, 4, 1)
    chip_queries(4)

    def ctx_unit():
        for k in range(1, 16):
            board.arrived(ctx_base + k, cbuf.at[(place.s - k + 16) % 16], place.sp_peer(16 - k))
        turned = cbuf[...].reshape(512, 256).astype(F32).T.astype(BF)
        for q in (0, 1):
            kvb[CTX_SLOT, q, 0:HEAD, :] = turned[0:HEAD, q * 256:(q + 1) * 256]
            kvb[CTX_SLOT, q, HEAD:HEAD + VDIM, :] = turned[128:128 + VDIM, q * 256:(q + 1) * 256]

    mark("m_init")
    m_ref[...] = jnp.full(m_ref.shape, -jnp.inf, F32)
    l_ref[...] = jnp.zeros(l_ref.shape, F32)
    acc[...] = jnp.zeros(acc.shape, F32)

    def products(slot, s_ref, mb_ref):
        for q in (0, 1):
            keys = kvb[slot, q, 0:128, :].T
            for n in range(4):
                cols = slice(n * 256, (n + 1) * 256)
                scores = jnp.dot(keys, qt[:, cols], preferred_element_type=F32)
                s_ref[q * 256:(q + 1) * 256, cols] = scores
                top = jnp.max(scores, axis=0, keepdims=True)
                mb_ref[:, cols] = top if q == 0 else jnp.maximum(mb_ref[:, cols], top)

    ones = jnp.ones((16, 256), BF)

    def absorb(slot, s_ref, mb_ref, bias):
        values = [jnp.concatenate([kvb[slot, q, HEAD:HEAD + VDIM, :], ones], axis=0)
                  for q in (0, 1)]
        for n in range(4):
            cols = slice(n * 256, (n + 1) * 256)
            old = m_ref[:, cols]
            top = mb_ref[:, cols] * SCALE2
            if bias is not None:
                top = top + bias
            new = jnp.maximum(old, top)
            m_ref[:, cols] = new
            factor = jnp.exp2(old - new)
            less = new if bias is None else new - bias
            weights = jnp.exp2(s_ref[:, cols] * SCALE2 - less)
            rounded = weights.astype(BF)
            summed = jnp.dot(values[0], rounded[:256], preferred_element_type=F32)
            summed = summed + jnp.dot(values[1], rounded[256:], preferred_element_type=F32)
            l_ref[:, cols] = l_ref[:, cols] * factor + summed[VDIM:VDIM + 1]
            acc[:, cols] = acc[:, cols] * factor + summed[:VDIM]

    ring_items = ring.items()
    ring_plan = [[] for _ in range(17)]
    for n, item in enumerate(ring_items):
        ring_plan[16 if n >= 12 else 1 + n].append(item)

    def actions(n):
        for key in PLAN[n]:
            kv_take(key)
        for item in ring_plan[n]:
            ring.take(*item)

    mark("n_prolog")
    actions(0)
    products(0, s_a, mb_a)
    for i in range(16):
        mark(f"o{i:02d}a")
        actions(i + 1)
        if i == 15:
            ctx_unit()
        mark(f"o{i:02d}b")
        products(2 * i + 1, s_b, mb_b)
        absorb(2 * i, s_a, mb_a, None)
        products(2 * i + 2, s_a, mb_a)
        absorb(2 * i + 1, s_b, mb_b, None)
    mark("p_last")
    bias = (bias_ref[0, 0] + math.log(TOK_DEV / CTX_DEV)) * LOG2E
    absorb(CTX_SLOT, s_a, mb_a, bias)

    mark("q_a2a")
    for k in range(8):
        cols = slice(k * 128, (k + 1) * 128)
        att[k] = (acc[:, cols] / l_ref[:, cols]).astype(BF)
    for k in (4, 3, 5, 2, 6, 1, 7):
        board.send(a2a_base + k, att.at[(place.z + k) % 8], attb.at[place.z], place.ring(k))
    attb[place.z] = att[place.z]
    for k in range(1, 8):
        board.arrived(a2a_base + k, attb.at[(place.z - k + 8) % 8], place.ring(-k))
    mark("r_out")
    rows = attb[...].reshape(8 * VDIM, 128).astype(F32).T.astype(BF)
    away_rows = pl.ds(pl.multiple_of(64 * (1 - place.c), 64), 64)
    for n, weight in enumerate((owa, owb)):
        part_ref[n] = jnp.dot(rows, weight[...].reshape(8 * VDIM, half_cols),
                              preferred_element_type=F32)
        board.send(d2d + n, part_ref.at[n, away_rows], sib_ref.at[n], place.sibling())
    mark("s_d2d")
    for n in (0, 1):
        cols = slice(n * half_cols, (n + 1) * half_cols)
        gates = jnp.concatenate([modf[k, 2:3, :] for k in range(8 * n, 8 * n + 8)], axis=1)
        mine = part_ref[n, pl.ds(pl.multiple_of(64 * place.c, 64), 64)]
        board.arrived(d2d + n, sib_ref.at[n], place.sibling())
        out_ref[:, cols] = (lat_ref[:, cols].astype(F32)
                            + gates * (mine + sib_ref[n])).astype(BF)

    mark("t_drain")
    for n in (0, 1):
        board.sent(d2d + n, sib_ref.at[n], place.sibling())
    for k in range(1, 8):
        board.sent(a2a_base + k, att.at[(place.z + k) % 8], place.ring(k))
    for k in range(1, 16):
        board.sent(ctx_base + k, cbuf.at[place.s], place.sp_peer(k))
    ring.drain()
    finish()
    for key in ITEM_ORDER:
        axis, step, _ = ITEMS[key]
        src = quarter_ref(kvb, 0, 0, key[4])
        board.sent(kv_base + ITEM_INDEX[key], src, place.plane(axis, step))
    mark(None)


def rotation_tables():
    frequency = np.power(np.float32(theta), -np.arange(8, dtype=np.float32) / np.float32(8))
    frequency = frequency.astype(np.float32).astype(np.float64)[:, None]
    token = np.arange(1024)[None, :]
    row, col = frequency * (token // GRID_W), frequency * (token % GRID_W)
    table = np.concatenate([np.cos(row), np.sin(row), np.cos(col), np.sin(col)])
    first = frequency * (np.arange(16)[None, :] * 16)
    base = np.stack([np.cos(first), np.sin(first)]).reshape(16, 16).T.reshape(256, 1)
    base = np.broadcast_to(base, (256, 128))
    return base.astype(np.float32), table.astype(np.float32)


def shards(
    latent,
    context,
    cond,
    cond_context,
    mod_weight,
    norm_gain,
    down_q,
    down_kv,
    rope_weight,
    qlat_gain,
    kvlat_gain,
    up_query,
    up_key,
    up_value,
    query_gain,
    key_gain,
    context_bias,
    out_weight,
):
    vmem = pl.BlockSpec(memory_space=pltpu.VMEM)
    smem = pl.BlockSpec(memory_space=pltpu.SMEM)
    copies = len(ITEM_ORDER) + 16 + 8 + 3 + 32 + 2 + 16 + 4 * 16 + 28
    base, table = rotation_tables()
    row = lambda v: v.reshape(1, -1)
    fold = lambda v: v.reshape(-1, 128)
    return pl.pallas_call(
        whole_kernel,
        out_shape=jax.ShapeDtypeStruct((64, D), BF),
        in_specs=[vmem] * 16 + [smem] + [vmem] * 3,
        out_specs=vmem,
        scratch_shapes=[
            pltpu.VMEM((8, 128, 768), BF),
            pltpu.VMEM((8, 128, 512), BF),
            pltpu.VMEM((64, D), BF),
            pltpu.VMEM((16, 8, 128), F32),
            pltpu.VMEM((16, 8, 128), F32),
            pltpu.VMEM((16, 160, 128), BF),
            pltpu.VMEM((160, 768), F32),
            pltpu.VMEM((160, 512), F32),
            pltpu.VMEM((64, 768), F32),
            pltpu.VMEM((96, 512), F32),
            pltpu.VMEM((16, 64, 768), BF),
            pltpu.VMEM((16, 64, 640), BF),
            pltpu.VMEM((160, 640), BF),
            pltpu.VMEM((ROPE, 1024), F32),
            pltpu.VMEM((128, 1024), BF),
            pltpu.VMEM((N_UNITS, 2, HEAD + VDIM, 256), BF),
            pltpu.VMEM((16, CTX_DEV, 256), BF),
            pltpu.VMEM((8, 64, D // 2), BF),
            pltpu.VMEM((8, 64, D // 2), BF),
            pltpu.VMEM((512, 1024), F32),
            pltpu.VMEM((512, 1024), F32),
            pltpu.VMEM((1, 1024), F32),
            pltpu.VMEM((1, 1024), F32),
            pltpu.VMEM((1, 1024), F32),
            pltpu.VMEM((1, 1024), F32),
            pltpu.VMEM((VDIM, 1024), F32),
            pltpu.VMEM((8, VDIM, 128), BF),
            pltpu.VMEM((8, VDIM, 128), BF),
            pltpu.VMEM((2, 128, D // 2), F32),
            pltpu.VMEM((2, 64, D // 2), F32),
            pltpu.SemaphoreType.DMA((copies,)),
            pltpu.SemaphoreType.DMA((copies,)),
        ],
        compiler_params=pltpu.CompilerParams(collective_id=0, has_side_effects=True,
                                             vmem_limit_bytes=56 * 1024 * 1024),
        name="whole",
    )(latent, context, fold(cond), fold(cond_context), mod_weight, fold(norm_gain), down_q, down_kv,
      rope_weight.T, fold(qlat_gain), fold(kvlat_gain), up_query.T, up_key.T, up_value.T, row(query_gain),
      row(key_gain), context_bias.reshape(1, 1), out_weight, jnp.asarray(base),
      jnp.asarray(table))


def solution(mesh):
    placed = (
        P(SP_TP, None),
        P("sp", None),
        P(),
        P(),
        P(None, "sp", "tp"),
        P(),
        P("tp", None),
        P("tp", None),
        P(),
        P(),
        P(),
        P(None, "tp"),
        P(None, "tp"),
        P(None, "tp"),
        P(),
        P(),
        P("tp"),
        P("tp", None),
    )
    return jax.shard_map(
        shards, mesh=mesh, in_specs=placed, out_specs=P(SP_TP, None), check_vma=False
    )
```
